256 devices in a mesh: grp: 2 (over y), fs: 16 (over z), tp: 8 (over x, core).
Axes of the slice: x: 4, y: 2, z: 16, core: 2. Of those that a mesh axis runs over, the one named last changes fastest.
The devices are a block of a 4x16x16 slice.
Arguments:
- stream: bfloat16 [2048, 12288], P('tp', ('grp', 'fs')), parts along dimension 1, may hold values from -6 to 6
- first_gain: float32 [2048], replicated, may hold values from 0.1 to 1.9
- first_gate: float32 [2048, 5632], P('fs', 'tp'), may hold values from -0.125 to 0.125
- first_gate_scale: float32 [5632], P('tp'), may hold values from 0.5 to 2
- first_up: float32 [2048, 5632], P('fs', 'tp'), may hold values from -0.125 to 0.125
- first_up_scale: float32 [5632], P('tp'), may hold values from 0.5 to 2
- first_down: float32 [5632, 2048], P('tp', 'fs'), may hold values from -0.078125 to 0.078125
- first_down_scale: float32 [2048], P('fs'), may hold values from 0.5 to 2
- mixer_gain: float32 [2048], replicated, may hold values from 0.1 to 1.9
- mixer_left: float32 [2048, 1024], P('fs', 'tp'), may hold values from -0.125 to 0.125
- mixer_left_scale: float32 [1024], P('tp'), may hold values from 0.5 to 2
- mixer_right: float32 [2048, 1024], P('fs', 'tp'), may hold values from -0.125 to 0.125
- mixer_right_scale: float32 [1024], P('tp'), may hold values from 0.5 to 2
- channel_gain: float32 [1024], P('tp'), may hold values from 0.1 to 1.9
- spatial: bfloat16 [8, 128, 128], P('tp'), may hold values from -0.5 to 0.5
- spatial_bias: float32 [8, 128], P('tp'), may hold values from 0.1 to 1.9
- mixer_out: float32 [1024, 2048], P('tp', 'fs'), may hold values from -0.1875 to 0.1875
- mixer_out_scale: float32 [2048], P('fs'), may hold values from 0.5 to 2
- second_gain: float32 [2048], replicated, may hold values from 0.1 to 1.9
- second_gate: float32 [2048, 5632], P('fs', 'tp'), may hold values from -0.125 to 0.125
- second_gate_scale: float32 [5632], P('tp'), may hold values from 0.5 to 2
- second_up: float32 [2048, 5632], P('fs', 'tp'), may hold values from -0.125 to 0.125
- second_up_scale: float32 [5632], P('tp'), may hold values from 0.5 to 2
- second_down: float32 [5632, 2048], P('tp', 'fs'), may hold values from -0.078125 to 0.078125
- second_down_scale: float32 [2048], P('fs'), may hold values from 0.5 to 2
Outputs:
- result: bfloat16 [2048, 12288], P('tp', ('grp', 'fs')), parts along dimension 1
The draws below stay inside these ranges and needn't reach their ends.
There are 2 independent parts, one for each index of `grp`. The reference program is written for one: setup_inputs(seed, part) draws one part's arguments, and reference() takes and returns one part's arrays. A program takes and returns all parts, laid end to end along the dimension named above; an argument that names none is the same for every part. Nothing has to cross between parts.
All inputs are finite; a program needn't handle non-finite values.
Results may differ from the reference program's by a relative error of at most 0.02.
Values may be sent and summed in bfloat16 or wider, within the bound.
A program may use at most 128 MiB of HBM per device.

```python
import math
import jax
import jax.numpy as jnp
from jax import lax

D = 2048
FF = 5632
BRANCH = 1024
GROUPS = 8
BLOCK = 128
TOKENS = 6144
N_TP = 8


def steps_of(rng, dims, split, least, largest):
    def one(axis_at, shards_of):
        draws = jax.random.uniform(jax.random.fold_in(jax.random.fold_in(rng, 6), axis_at), (shards_of,), jnp.float32, least / len(split), largest / len(split))
        return jnp.repeat(jnp.exp(draws), dims[axis_at] // shards_of).reshape((-1,) + (1,) * (len(dims) - axis_at - 1))

    level = one(*split[0])
    for cut in split[1:]:
        level = level * one(*cut)
    return level


def normal_values(own_key, shape, scale, most, split=(), kind=jnp.bfloat16):
    values = jax.random.normal(own_key, shape, jnp.float32) * scale
    if len(split) > 0:
        values = steps_of(own_key, shape, split, -0.22, 0.18) * values
    return jnp.clip(values, min=-most, max=most).astype(kind)


def setup_inputs(seed: int = 0, part: int = 0) -> dict:
    key_of = jax.random.split(jax.random.key(seed), 26)
    own_keys = jax.random.split(jax.random.fold_in(key_of[25], part), 26)
    return {
        "stream": normal_values(own_keys[0], (D, TOKENS), 1.0, 6.0, ((0, 8), (1, 16))),
        "first_gain": jnp.clip(1.0 + 0.18 * jax.random.normal(key_of[1], (D,), jnp.float32), 0.1, 1.9),
        "first_gate": normal_values(key_of[2], (D, FF), D ** -0.5, 0.125, ((0, 16), (1, 8)), jnp.float32),
        "first_gate_scale": jnp.clip(jnp.exp(math.log(2.0) - 1.3862944 * jax.random.uniform(key_of[3], (FF,), jnp.float32) ** steps_of(key_of[3], (FF,), ((0, 8),), -0.2, 0.2)), 0.5, 2.0),
        "first_up": normal_values(key_of[4], (D, FF), D ** -0.5, 0.125, ((0, 16), (1, 8)), jnp.float32),
        "first_up_scale": jnp.clip(jnp.exp(math.log(2.0) - 1.3862944 * jax.random.uniform(key_of[5], (FF,), jnp.float32) ** steps_of(key_of[5], (FF,), ((0, 8),), -0.2, 0.2)), 0.5, 2.0),
        "first_down": normal_values(key_of[6], (FF, D), FF ** -0.5, 0.078125, ((0, 8), (1, 16)), jnp.float32),
        "first_down_scale": jnp.clip(jnp.exp(math.log(2.0) - 1.3862944 * jax.random.uniform(key_of[7], (D,), jnp.float32) ** steps_of(key_of[7], (D,), ((0, 16),), -0.2, 0.2)), 0.5, 2.0),
        "mixer_gain": jnp.clip(1.0 + 0.18 * jax.random.normal(key_of[8], (D,), jnp.float32), 0.1, 1.9),
        "mixer_left": normal_values(key_of[9], (D, BRANCH), D ** -0.5, 0.125, ((0, 16), (1, 8)), jnp.float32),
        "mixer_left_scale": jnp.clip(jnp.exp(math.log(2.0) - 1.3862944 * jax.random.uniform(key_of[10], (BRANCH,), jnp.float32) ** steps_of(key_of[10], (BRANCH,), ((0, 8),), -0.2, 0.2)), 0.5, 2.0),
        "mixer_right": normal_values(key_of[11], (D, BRANCH), D ** -0.5, 0.125, ((0, 16), (1, 8)), jnp.float32),
        "mixer_right_scale": jnp.clip(jnp.exp(math.log(2.0) - 1.3862944 * jax.random.uniform(key_of[12], (BRANCH,), jnp.float32) ** steps_of(key_of[12], (BRANCH,), ((0, 8),), -0.2, 0.2)), 0.5, 2.0),
        "channel_gain": jnp.clip(1.0 + 0.18 * jax.random.normal(key_of[13], (BRANCH,), jnp.float32), 0.1, 1.9),
        "spatial": normal_values(key_of[14], (GROUPS, BLOCK, BLOCK), BLOCK ** -0.5, 0.5, ((0, 8),)),
        "spatial_bias": jnp.clip(1.0 + 0.18 * jax.random.normal(key_of[15], (GROUPS, BLOCK), jnp.float32), 0.1, 1.9),
        "mixer_out": normal_values(key_of[16], (BRANCH, D), BRANCH ** -0.5, 0.1875, ((0, 8), (1, 16)), jnp.float32),
        "mixer_out_scale": jnp.clip(jnp.exp(math.log(2.0) - 1.3862944 * jax.random.uniform(key_of[17], (D,), jnp.float32) ** steps_of(key_of[17], (D,), ((0, 16),), -0.2, 0.2)), 0.5, 2.0),
        "second_gain": jnp.clip(1.0 + 0.18 * jax.random.normal(key_of[18], (D,), jnp.float32), 0.1, 1.9),
        "second_gate": normal_values(key_of[19], (D, FF), D ** -0.5, 0.125, ((0, 16), (1, 8)), jnp.float32),
        "second_gate_scale": jnp.clip(jnp.exp(math.log(2.0) - 1.3862944 * jax.random.uniform(key_of[20], (FF,), jnp.float32) ** steps_of(key_of[20], (FF,), ((0, 8),), -0.2, 0.2)), 0.5, 2.0),
        "second_up": normal_values(key_of[21], (D, FF), D ** -0.5, 0.125, ((0, 16), (1, 8)), jnp.float32),
        "second_up_scale": jnp.clip(jnp.exp(math.log(2.0) - 1.3862944 * jax.random.uniform(key_of[22], (FF,), jnp.float32) ** steps_of(key_of[22], (FF,), ((0, 8),), -0.2, 0.2)), 0.5, 2.0),
        "second_down": normal_values(key_of[23], (FF, D), FF ** -0.5, 0.078125, ((0, 8), (1, 16)), jnp.float32),
        "second_down_scale": jnp.clip(jnp.exp(math.log(2.0) - 1.3862944 * jax.random.uniform(key_of[24], (D,), jnp.float32) ** steps_of(key_of[24], (D,), ((0, 16),), -0.2, 0.2)), 0.5, 2.0),
    }


EPS = 1e-06

def rms_rows(stream, gain):
    values = stream.astype(jnp.float32)
    inverse = lax.rsqrt(lax.optimization_barrier(jnp.mean(values * values, axis=0)) + EPS)
    return (values * inverse * gain[:, None]).astype(jnp.bfloat16)

def project(weight, scale, inputs):
    product = lax.dot_general(weight.astype(jnp.bfloat16), inputs, (((0,), (0,)), ((), ())), preferred_element_type=jnp.float32)
    return product * scale[:, None]

def block_sum(weight, scale, hidden):
    width = weight.shape[0] // N_TP
    total = jnp.zeros((weight.shape[1], hidden.shape[1]), jnp.float32)
    for index in range(N_TP):
        term = project(weight[index * width:(index + 1) * width], scale, hidden[index * width:(index + 1) * width])
        total = total + lax.optimization_barrier(term.astype(jnp.bfloat16)).astype(jnp.float32)
    return total

def half_step(stream, gain, gate_weight, gate_scale, up_weight, up_scale, down_weight, down_scale):
    normed_rows = rms_rows(stream, gain)
    gate = project(gate_weight, gate_scale, normed_rows)
    upward = project(up_weight, up_scale, normed_rows)
    hidden = (jax.nn.silu(gate) * upward).astype(jnp.bfloat16)
    total = block_sum(down_weight, down_scale, hidden)
    return (stream.astype(jnp.float32) + 0.5 * total).astype(jnp.bfloat16)

def reference(stream, first_gain, first_gate, first_gate_scale, first_up, first_up_scale, first_down, first_down_scale, mixer_gain, mixer_left, mixer_left_scale, mixer_right, mixer_right_scale, channel_gain, spatial, spatial_bias, mixer_out, mixer_out_scale, second_gain, second_gate, second_gate_scale, second_up, second_up_scale, second_down, second_down_scale):
    stream = half_step(stream, first_gain, first_gate, first_gate_scale, first_up, first_up_scale, first_down, first_down_scale)
    normed_rows = rms_rows(stream, mixer_gain)
    left = jax.nn.gelu(project(mixer_left, mixer_left_scale, normed_rows))
    right = jax.nn.gelu(project(mixer_right, mixer_right_scale, normed_rows))
    average = lax.optimization_barrier(jnp.mean(right, axis=0))
    squares = lax.optimization_barrier(jnp.mean(right * right, axis=0))
    inverse = lax.rsqrt(squares - average * average + EPS)
    centred = ((right - average) * inverse * channel_gain[:, None]).astype(jnp.bfloat16)
    blocks = centred.reshape(GROUPS, BRANCH // GROUPS, TOKENS // BLOCK, BLOCK)
    lower = jnp.tril(jnp.ones((BLOCK, BLOCK), dtype=bool))
    masked = jnp.where(lower[None], spatial, jnp.zeros_like(spatial))
    token_mix = jnp.einsum('gts,gcns->gcnt', masked.astype(jnp.float32), blocks.astype(jnp.float32))
    token_mix = token_mix + spatial_bias[:, None, None, :]
    gated = (left * token_mix.reshape(BRANCH, TOKENS)).astype(jnp.bfloat16)
    total = block_sum(mixer_out, mixer_out_scale, gated)
    stream = (stream.astype(jnp.float32) + total).astype(jnp.bfloat16)
    return half_step(stream, second_gain, second_gate, second_gate_scale, second_up, second_up_scale, second_down, second_down_scale)
```

```python
import jax
import jax.numpy as jnp
from jax import lax
from jax.experimental import pallas as pl
from jax.experimental.pallas import tpu as pltpu
from jax.sharding import PartitionSpec as P

MESH = pl.DeviceIdType.MESH
EPS = 1e-06
F32, BF16 = jnp.float32, jnp.bfloat16
LANES = 128


def contract_rows(a, b):
    return lax.dot_general(a, b, (((0,), (0,)), ((), ())), preferred_element_type=F32)


def kernel(
    sizes,
    stream_ref,
    pack_ref,
    scale_ref,
    gains_ref,
    hidden_scales_ref,
    mixer_cols_ref,
    spatial_ref,
    bias_ref,
    out_ref,
    w,
    scl,
    act,
    xn,
    acc,
    hid,
    gated,
    left,
    right,
    pbuf,
    sb,
    pr,
    cb,
    rr,
    st,
    st_own,
    in_sem,
    zsend,
    zrecv,
    ssend,
    srecv,
    ysend,
    yrecv,
    psend,
    precv,
    csend,
    crecv,
    gsend,
    grecv,
    tsend,
    trecv,
):
    nz, ntp, ff, ch, span = sizes
    nx, half = ntp // 2, nz // 2
    rows, toks = stream_ref.shape
    g, z, t = lax.axis_index("grp"), lax.axis_index("fs"), lax.axis_index("tp")
    x, c = t // 2, t % 2
    gp = g % 2

    def at_tp(other):
        return (g, z, other)

    partner = (g + 1 - 2 * gp, z, t)
    sibling = at_tp(2 * x + 1 - c)
    xr, xl = (x + 1) % nx, (x + nx - 1) % nx
    right_x, left_x = at_tp(2 * xr + c), at_tp(2 * xl + c)
    around = ((g, (z + 1) % nz, t), (g, (z + nz - 1) % nz, t))

    def copy(src, dst, send, recv, device):
        return pltpu.make_async_remote_copy(
            src_ref=src, dst_ref=dst, send_sem=send, recv_sem=recv, device_id=device, device_id_type=MESH
        )

    third = ff * 15 // 44
    alone = (2 * third, third, ch, 2 * third, third)
    total = (2 * ff, ff, 3 * ch, 2 * ff, ff)
    base, first = [], 0
    for n in total:
        base.append(first)
        first += n

    def part(p, sub, zs):
        shared = total[p] - 2 * alone[p]
        if sub == 0:
            return w.at[zs, pl.ds(pl.multiple_of(base[p] + gp * (alone[p] + shared), 16), alone[p])]
        return w.at[zs, pl.ds(base[p] + alone[p], shared)]

    def other_part(p, zs):
        shared = total[p] - 2 * alone[p]
        return w.at[zs, pl.ds(pl.multiple_of(base[p] + (1 - gp) * (alone[p] + shared), 16), alone[p])]

    def source(d, k):
        return (z + nz - k) % nz if d == 0 else (z + k) % nz

    def last(d, sub):
        return half if d == sub else half - 1

    def hop(p, d, sub, zs, k):
        return copy(part(p, sub, zs), part(p, sub, zs), zsend.at[p, d, sub, k], zrecv.at[p, d, sub, k], around[d])

    def scale_hop(d, zs, k):
        return copy(scl.at[zs], scl.at[zs], ssend.at[d, k], srecv.at[d, k], around[d])

    def across(p, zs):
        return copy(part(p, 0, zs), part(p, 0, zs), ysend.at[p, zs], yrecv.at[p, zs], partner)

    def start_ring(p):
        for sub in (0, 1):
            for d in (0, 1):
                hop(p, d, sub, z, 0).start()

    def tick(p, k):
        for sub in (0, 1):
            for d in (0, 1):
                zs = source(d, k)

                @pl.when(k <= last(d, sub))
                def _():
                    hop(p, d, sub, zs, k - 1).wait_recv()

                @pl.when(k < last(d, sub))
                def _():
                    hop(p, d, sub, zs, k).start()

                if sub == 0:

                    @pl.when(k <= last(d, sub))
                    def _():
                        across(p, zs).start()

    def scale_tick(k):
        for d in (0, 1):
            zs = source(d, k)

            @pl.when(k <= last(d, 0))
            def _():
                scale_hop(d, zs, k - 1).wait_recv()

            @pl.when(k < last(d, 0))
            def _():
                scale_hop(d, zs, k).start()

    def pair_of(j):
        return (z + nz - j % half) % nz, (z + j) % nz

    def wait_across(p, j):
        for zs in pair_of(j):

            @pl.when(zs != z)
            def _():
                copy(other_part(p, zs), other_part(p, zs), ysend.at[p, zs], yrecv.at[p, zs], partner).wait_recv()

    own_rows = pl.ds(pl.multiple_of(t * rows, rows), rows)
    hr = rows // 2

    def chunk(r, tt, h):
        return act.at[r, pl.ds(pl.multiple_of(tt * rows + h * hr, hr), hr)]

    def g_half(r, i, tt, h, device):
        return copy(chunk(r, tt, h), chunk(r, tt, h), gsend.at[r, i], grecv.at[r, i], device)

    def g_whole(r):
        return copy(act.at[r, own_rows], act.at[r, own_rows], gsend.at[r, 0], grecv.at[r, 0], sibling)

    far = (x + 2) % nx

    def gather_start(r):
        g_half(r, 1, t, 0, right_x).start()
        g_half(r, 4, t, 1, left_x).start()
        g_half(r, 2, t, 1, right_x).start()
        g_half(r, 3, t, 0, left_x).start()
        g_whole(r).start()

    def gather_middle(r):
        from_left, from_right = 2 * xl + c, 2 * xr + c
        g_half(r, 1, from_left, 0, right_x).wait_recv()
        g_half(r, 5, from_left, 0, right_x).start()
        g_half(r, 7, from_left, 0, sibling).start()
        g_half(r, 4, from_right, 1, left_x).wait_recv()
        g_half(r, 6, from_right, 1, left_x).start()
        g_half(r, 10, from_right, 1, sibling).start()
        g_half(r, 2, from_left, 1, right_x).wait_recv()
        g_half(r, 8, from_left, 1, sibling).start()
        g_half(r, 3, from_right, 0, left_x).wait_recv()
        g_half(r, 9, from_right, 0, sibling).start()

    def gather_end(r):
        o = 1 - c
        g_half(r, 5, 2 * far + c, 0, right_x).wait_recv()
        g_half(r, 11, 2 * far + c, 0, sibling).start()
        g_half(r, 6, 2 * far + c, 1, left_x).wait_recv()
        g_half(r, 12, 2 * far + c, 1, sibling).start()
        g_whole(r).wait_recv()
        for i, xs, h in ((7, xl, 0), (8, xl, 1), (9, xr, 0), (10, xr, 1), (11, far, 0), (12, far, 1)):
            g_half(r, i, 2 * xs + o, h, sibling).wait_recv()

    def gather_drain(r):
        g_whole(r).wait_send()
        for i in range(1, 13):
            g_half(r, i, t, 0, sibling).wait_send()

    def normalise(r):
        def squares(i, s):
            v = act[r, pl.ds(pl.multiple_of(i * LANES, LANES), LANES)].astype(F32)
            return s + jnp.sum(v * v, axis=0, keepdims=True)

        s = lax.fori_loop(0, nz, squares, jnp.zeros((1, toks), F32))
        inverse = lax.rsqrt(s / (rows * ntp) + EPS)

        def apply(i, _):
            at = pl.ds(pl.multiple_of(i * LANES, LANES), LANES)
            v = act[r, at].astype(F32)
            xn[at] = (v * inverse * gains_ref[at, r : r + 1]).astype(BF16)
            return 0

        lax.fori_loop(0, nz, apply, 0)

    def project_pair(at, n, j, piece):
        a, b = pair_of(j)
        rhs = jnp.concatenate(
            [xn[pl.ds(pl.multiple_of(q * LANES, LANES), LANES)] for q in (a, b)], axis=0
        )

        def one(i, _):
            here = pl.ds(pl.multiple_of(at + i * piece, 16), piece)
            lhs = jnp.concatenate([w[a, here], w[b, here]], axis=1)
            got = jnp.dot(lhs, rhs, preferred_element_type=F32)
            there = pl.ds(pl.multiple_of(i * piece, 16), piece)
            acc[there] = acc[there] + got
            return 0

        lax.fori_loop(0, n // piece, one, 0)

    def clear(n):
        def one(i, _):
            acc[pl.ds(pl.multiple_of(i * 64, 64), 64)] = jnp.zeros((64, toks), F32)
            return 0

        lax.fori_loop(0, n // 64, one, 0)

    def hidden(b):
        def one(i, _):
            at = pl.ds(pl.multiple_of(i * 64, 64), 64)
            up_at = pl.ds(pl.multiple_of(ff + i * 64, 64), 64)
            gate = acc[at] * hidden_scales_ref[at, 2 * b : 2 * b + 1]
            up = acc[up_at] * hidden_scales_ref[at, 2 * b + 1 : 2 * b + 2]
            hid[at] = (gate / (1.0 + jnp.exp(-gate)) * up).astype(BF16)
            return 0

        lax.fori_loop(0, ff // 64, one, 0)

    def to_sibling(r, zs):
        return copy(sb.at[r, zs], pr.at[r, zs], psend.at[r, zs], precv.at[r, zs], sibling)

    def to_owner(r, zs):
        return copy(
            cb.at[r, zs],
            rr.at[r, x, zs % 2],
            csend.at[r, zs],
            crecv.at[r, x, zs % 2],
            at_tp(2 * (zs // 4) + c),
        )

    def produce(r, j, lhs, rhs):
        product = contract_rows(lhs, rhs)
        for i, zs in enumerate(pair_of(j)):
            col = jnp.transpose(scl[zs])[:, r : r + 1]
            term = product[i * LANES : (i + 1) * LANES] * col
            mine = (zs // 2) % 2 == c

            @pl.when(mine)
            def _():
                pbuf[zs] = term

            @pl.when(jnp.logical_not(mine))
            def _():
                sb[r, zs] = term.astype(BF16)
                to_sibling(r, zs).start()

    def combine(r, j):
        for zs in pair_of(j):

            @pl.when((zs // 2) % 2 == c)
            def _():
                to_sibling(r, zs).wait_recv()
                both = (pbuf[zs] + pr[r, zs].astype(F32)).astype(BF16)

                @pl.when(zs // 4 == x)
                def _():
                    rr[r, x, zs % 2] = both

                @pl.when(zs // 4 != x)
                def _():
                    cb[r, zs] = both
                    to_owner(r, zs).start()

    def finish(r, factor):
        for xs in range(nx):

            @pl.when(xs != x)
            def _():
                for h in (0, 1):
                    copy(cb.at[r, 0], rr.at[r, xs, h], csend.at[r, 0], crecv.at[r, xs, h], sibling).wait_recv()

        news = []
        for h in (0, 1):
            summed = rr[r, 0, h].astype(F32)
            for xs in range(1, nx):
                summed = summed + rr[r, xs, h].astype(F32)
            at = pl.ds(pl.multiple_of(t * rows + h * LANES, LANES), LANES)
            news.append((act[r, at].astype(F32) + factor * summed).astype(BF16))
        return news

    def next_stream(r, factor):
        for h, new in enumerate(finish(r, factor)):
            act[r + 1, pl.ds(pl.multiple_of(t * rows + h * LANES, LANES), LANES)] = new

    def reduce_drain(r):
        def one(zs, _):
            @pl.when((zs // 2) % 2 != c)
            def _():
                to_sibling(r, zs).wait_send()

            @pl.when(jnp.logical_and((zs // 2) % 2 == c, zs // 4 != x))
            def _():
                to_owner(r, zs).wait_send()

            return 0

        lax.fori_loop(0, nz, one, 0)

    def down_piece(p, r, j):
        a, b = pair_of(j)
        lhs = jnp.concatenate([w[a, pl.ds(base[p], ff)], w[b, pl.ds(base[p], ff)]], axis=1)
        produce(r, j, lhs, hid[...])

    fetch_stream = pltpu.make_async_copy(stream_ref, act.at[0, own_rows], in_sem.at[0])
    fetch_scale = pltpu.make_async_copy(scale_ref, scl.at[z], in_sem.at[1])
    fetches = [
        pltpu.make_async_copy(
            pack_ref.at[pl.ds(base[p], total[p])], w.at[z, pl.ds(base[p], total[p])], in_sem.at[2 + p]
        )
        for p in range(5)
    ]
    fetches[0].start()
    fetch_stream.start()
    fetch_scale.start()
    for p in range(1, 5):
        fetches[p].start()

    barrier = pltpu.get_barrier_semaphore()
    peers = [*around, partner] + [at_tp((t + d) % ntp) for d in range(1, ntp)]
    for device in peers:
        pl.semaphore_signal(barrier, inc=1, device_id=device, device_id_type=MESH)
    pl.semaphore_wait(barrier, len(peers))

    fetches[0].wait()
    start_ring(0)
    fetch_stream.wait()
    gather_start(0)
    fetch_scale.wait()
    for d in (0, 1):
        scale_hop(d, z, 0).start()
    for p in range(1, 5):
        fetches[p].wait()
    clear(2 * ff)
    tick(0, 1)
    gather_middle(0)
    scale_tick(1)
    tick(0, 2)
    gather_end(0)
    normalise(0)

    def first_loop(j, _):
        @pl.when(j + 2 <= half)
        def _():
            tick(0, j + 2)
            scale_tick(j + 1)

        @pl.when(j + 2 == half - 1)
        def _():
            start_ring(1)
            start_ring(2)

        wait_across(0, j)
        project_pair(base[0], 2 * ff, j, ff // 2)
        return 0

    lax.fori_loop(1, half + 1, first_loop, 0)
    scale_tick(half)
    hidden(0)
    tick(1, 1)
    tick(2, 1)

    def second_loop(j, _):
        @pl.when(j + 1 <= half)
        def _():
            tick(1, j + 1)
            tick(2, j + 1)

        @pl.when(j + 1 == half - 1)
        def _():
            start_ring(3)

        wait_across(1, j)
        down_piece(1, 0, j)

        @pl.when(j > 1)
        def _():
            combine(0, j - 1)

        return 0

    lax.fori_loop(1, half + 1, second_loop, 0)
    combine(0, half)
    tick(3, 1)
    next_stream(0, 0.5)
    gather_start(1)
    tick(3, 2)
    gather_middle(1)
    tick(3, 3)
    gather_end(1)
    normalise(1)
    clear(2 * ch)

    def mixer_loop(j, _):
        wait_across(2, j)
        project_pair(base[2], 2 * ch, j, 2 * ch)
        return 0

    lax.fori_loop(1, half + 1, mixer_loop, 0)
    left[...] = jax.nn.gelu(acc[0:ch] * mixer_cols_ref[:, 0:1])
    right[...] = jax.nn.gelu(acc[ch : 2 * ch] * mixer_cols_ref[:, 1:2])
    st_own[...] = jnp.zeros_like(st_own)
    st_own[0:1] = jnp.sum(right[...], axis=0, keepdims=True)
    st_own[1:2] = jnp.sum(right[...] * right[...], axis=0, keepdims=True)

    def to_peer(d):
        return copy(st_own, st.at[t], tsend.at[d - 1], trecv.at[t], at_tp((t + d) % ntp))

    def from_peer(d):
        src = (t + d) % ntp
        return copy(st_own, st.at[src], tsend.at[d - 1], trecv.at[src], at_tp(src))

    for d in range(1, ntp):
        to_peer(d).start()
    tick(3, 4)
    st[t] = st_own[...]
    for d in range(1, ntp):
        from_peer(d).wait_recv()
    sums = st[0]
    for i in range(1, ntp):
        sums = sums + st[i]
    average = sums[0:1] / (ch * ntp)
    inverse = lax.rsqrt(sums[1:2] / (ch * ntp) - average * average + EPS)
    centred = ((right[...] - average) * inverse * mixer_cols_ref[:, 2:3]).astype(BF16)
    target = lax.broadcasted_iota(jnp.int32, (span, span), 0)
    origin = lax.broadcasted_iota(jnp.int32, (span, span), 1)
    masked = jnp.where(origin <= target, spatial_ref[...].astype(F32), 0.0).astype(BF16)
    for n in range(toks // span):
        at = slice(n * span, (n + 1) * span)
        mixed = lax.dot_general(
            centred[:, at], masked, (((1,), (1,)), ((), ())), preferred_element_type=F32
        )
        gated[:, at] = (left[:, at] * (mixed + bias_ref[...])).astype(BF16)

    def mixer_out_loop(j, _):
        a, b = pair_of(j)
        here = pl.ds(base[2] + 2 * ch, ch)
        produce(1, j, jnp.concatenate([w[a, here], w[b, here]], axis=1), gated[...])

        @pl.when(j > 1)
        def _():
            combine(1, j - 1)

        return 0

    lax.fori_loop(1, half + 1, mixer_out_loop, 0)
    combine(1, half)
    tick(3, 5)
    next_stream(1, 1.0)
    gather_start(2)
    tick(3, 6)
    gather_middle(2)
    start_ring(4)
    tick(3, 7)
    gather_end(2)
    normalise(2)
    clear(2 * ff)
    tick(3, 8)
    early = 3

    def third_loop(j, _):
        @pl.when(j % 2 == 1)
        def _():
            @pl.when((j + 1) // 2 <= early)
            def _():
                tick(4, (j + 1) // 2)

        wait_across(3, j)
        project_pair(base[3], 2 * ff, j, ff // 2)
        return 0

    lax.fori_loop(1, half + 1, third_loop, 0)
    hidden(1)

    def fourth_loop(j, _):
        @pl.when(j + early <= half)
        def _():
            tick(4, j + early)

        wait_across(4, j)
        down_piece(4, 2, j)

        @pl.when(j > 1)
        def _():
            combine(2, j - 1)

        return 0

    lax.fori_loop(1, half + 1, fourth_loop, 0)
    combine(2, half)
    for h, new in enumerate(finish(2, 0.5)):
        out_ref[h * LANES : (h + 1) * LANES] = new

    def drain(k, _):
        for p in range(5):
            for sub in (0, 1):
                for d in (0, 1):

                    @pl.when(k < last(d, sub))
                    def _():
                        hop(p, d, sub, z, k).wait_send()

            for zs in (2 * k, 2 * k + 1):

                @pl.when(zs != z)
                def _():
                    across(p, zs).wait_send()
        for d in (0, 1):

            @pl.when(k < last(d, 0))
            def _():
                scale_hop(d, z, k).wait_send()

        return 0

    lax.fori_loop(0, half, drain, 0)
    for r in range(3):
        gather_drain(r)
        reduce_drain(r)
    for d in range(1, ntp):
        to_peer(d).wait_send()


def solution(mesh):
    nz, ntp = mesh.shape["fs"], mesh.shape["tp"]

    def local(
        stream,
        first_gain,
        first_gate,
        first_gate_scale,
        first_up,
        first_up_scale,
        first_down,
        first_down_scale,
        mixer_gain,
        mixer_left,
        mixer_left_scale,
        mixer_right,
        mixer_right_scale,
        channel_gain,
        spatial,
        spatial_bias,
        mixer_out,
        mixer_out_scale,
        second_gain,
        second_gate,
        second_gate_scale,
        second_up,
        second_up_scale,
        second_down,
        second_down_scale,
    ):
        rows, toks = stream.shape
        width, ff = first_gate.shape
        ch, span = mixer_left.shape[1], spatial.shape[1]
        whole = width * nz
        pack = jnp.concatenate(
            [
                first_gate.T,
                first_up.T,
                first_down,
                mixer_left.T,
                mixer_right.T,
                mixer_out,
                second_gate.T,
                second_up.T,
                second_down,
            ],
            axis=0,
        ).astype(BF16)
        scales = jnp.stack([first_down_scale, mixer_out_scale, second_down_scale] + [second_down_scale] * 5)
        gains = jnp.stack([first_gain, mixer_gain, second_gain], axis=1)
        hidden_scales = jnp.stack(
            [first_gate_scale, first_up_scale, second_gate_scale, second_up_scale], axis=1
        )
        mixer_cols = jnp.stack([mixer_left_scale, mixer_right_scale, channel_gain], axis=1)
        depth = pack.shape[0]
        dma, half = pltpu.SemaphoreType.DMA, nz // 2
        vmem, anywhere = pl.BlockSpec(memory_space=pltpu.VMEM), pl.BlockSpec(memory_space=pl.ANY)
        sizes = (nz, ntp, ff, ch, span)

        def body(*refs):
            kernel(sizes, *refs)

        piece = (nz, LANES, toks)
        return pl.pallas_call(
            body,
            out_shape=jax.ShapeDtypeStruct((rows, toks), BF16),
            in_specs=[anywhere, anywhere, anywhere] + [vmem] * 5,
            out_specs=vmem,
            scratch_shapes=[
                pltpu.VMEM((nz, depth, LANES), BF16),
                pltpu.VMEM((nz, 8, LANES), F32),
                pltpu.VMEM((3, whole, toks), BF16),
                pltpu.VMEM((whole, toks), BF16),
                pltpu.VMEM((2 * ff, toks), F32),
                pltpu.VMEM((ff, toks), BF16),
                pltpu.VMEM((ch, toks), BF16),
                pltpu.VMEM((ch, toks), F32),
                pltpu.VMEM((ch, toks), F32),
                pltpu.VMEM(piece, F32),
                pltpu.VMEM((3, *piece), BF16),
                pltpu.VMEM((3, *piece), BF16),
                pltpu.VMEM((3, *piece), BF16),
                pltpu.VMEM((3, ntp // 2, 2, LANES, toks), BF16),
                pltpu.VMEM((ntp, 8, toks), F32),
                pltpu.VMEM((8, toks), F32),
                dma((7,)),
                dma((5, 2, 2, half)),
                dma((5, 2, 2, half)),
                dma((2, half)),
                dma((2, half)),
                dma((5, nz)),
                dma((5, nz)),
                dma((3, nz)),
                dma((3, nz)),
                dma((3, nz)),
                dma((3, ntp // 2, 2)),
                dma((3, 13)),
                dma((3, 13)),
                dma((ntp,)),
                dma((ntp,)),
            ],
            compiler_params=pltpu.CompilerParams(
                collective_id=0, has_side_effects=True, vmem_limit_bytes=60 * 1024 * 1024
            ),
            name="layer",
        )(stream, pack, scales, gains, hidden_scales, mixer_cols, spatial.reshape(span, span), spatial_bias)

    return jax.shard_map(
        local,
        mesh=mesh,
        in_specs=(
            P("tp", ("grp", "fs")),
            P(),
            P("fs", "tp"),
            P("tp"),
            P("fs", "tp"),
            P("tp"),
            P("tp", "fs"),
            P("fs"),
            P(),
            P("fs", "tp"),
            P("tp"),
            P("fs", "tp"),
            P("tp"),
            P("tp"),
            P("tp", None, None),
            P("tp", None),
            P("tp", "fs"),
            P("fs"),
            P(),
            P("fs", "tp"),
            P("tp"),
            P("fs", "tp"),
            P("tp"),
            P("tp", "fs"),
            P("fs"),
        ),
        out_specs=P("tp", ("grp", "fs")),
        check_vma=False,
    )
```

```python
import jax
import jax.numpy as jnp
from jax import lax
from jax.experimental import pallas as pl
from jax.experimental.pallas import tpu as pltpu
from jax.sharding import PartitionSpec as P

MESH = pl.DeviceIdType.MESH
EPS = 1e-06
F32, BF16 = jnp.float32, jnp.bfloat16
LANES = 128


def contract_rows(a, b):
    return lax.dot_general(a, b, (((0,), (0,)), ((), ())), preferred_element_type=F32)


def kernel(
    sizes,
    stream_ref,
    pack_ref,
    vectors_ref,
    spatial_ref,
    bias_ref,
    out_ref,
    w,
    scl,
    cols,
    act,
    xn,
    acc,
    hid,
    gated,
    left,
    right,
    pbuf,
    sb,
    pr,
    cb,
    rr,
    st,
    st_own,
    in_sem,
    zsend,
    zrecv,
    ssend,
    srecv,
    ysend,
    yrecv,
    psend,
    precv,
    csend,
    crecv,
    gsend,
    grecv,
    tsend,
    trecv,
):
    nz, ntp, ff, ch, span = sizes
    nx, half = ntp // 2, nz // 2
    hidden_at = vectors_ref.shape[1] - 2 * LANES - (-ff % LANES) - ff
    mixer_at = vectors_ref.shape[1] - 2 * LANES
    scale_at = vectors_ref.shape[1] - LANES
    rows, toks = stream_ref.shape
    g, z, t = lax.axis_index("grp"), lax.axis_index("fs"), lax.axis_index("tp")
    x, c = t // 2, t % 2
    gp = g % 2

    def at_tp(other):
        return (g, z, other)

    partner = (g + 1 - 2 * gp, z, t)
    sibling = at_tp(2 * x + 1 - c)
    xr, xl = (x + 1) % nx, (x + nx - 1) % nx
    right_x, left_x = at_tp(2 * xr + c), at_tp(2 * xl + c)
    around = ((g, (z + 1) % nz, t), (g, (z + nz - 1) % nz, t))

    def copy(src, dst, send, recv, device):
        return pltpu.make_async_remote_copy(
            src_ref=src, dst_ref=dst, send_sem=send, recv_sem=recv, device_id=device, device_id_type=MESH
        )

    third = ff * 15 // 44
    alone = (2 * third, third, ch, 2 * third, third)
    total = (2 * ff, ff, 3 * ch, 2 * ff, ff)
    base, first = [], 0
    for n in total:
        base.append(first)
        first += n

    def part(p, sub, zs):
        shared = total[p] - 2 * alone[p]
        if sub == 0:
            return w.at[zs, pl.ds(pl.multiple_of(base[p] + gp * (alone[p] + shared), 16), alone[p])]
        return w.at[zs, pl.ds(base[p] + alone[p], shared)]

    def source(d, k):
        return (z + nz - k) % nz if d == 0 else (z + k) % nz

    def last(d, sub):
        return half if d == sub else half - 1

    def hop(p, d, sub, zs, k):
        return copy(part(p, sub, zs), part(p, sub, zs), zsend.at[p], zrecv.at[p, d, sub, k], around[d])

    def scale_hop(d, zs, k):
        return copy(scl.at[zs], scl.at[zs], ssend.at[0], srecv.at[d, k], around[d])

    def across(p, zs, k):
        return copy(part(p, 0, zs), part(p, 0, zs), ysend.at[p], yrecv.at[p, k - 1], partner)

    def start_ring(p):
        for sub in (0, 1):
            for d in (0, 1):
                hop(p, d, sub, z, 0).start()

    def tick(p, k):
        for sub in (0, 1):
            for d in (0, 1):
                zs = source(d, k)

                @pl.when(k <= last(d, sub))
                def _():
                    hop(p, d, sub, zs, k - 1).wait_recv()

                @pl.when(k < last(d, sub))
                def _():
                    hop(p, d, sub, zs, k).start()

                if sub == 0:

                    @pl.when(k <= last(d, sub))
                    def _():
                        across(p, zs, k).start()

    def scale_tick(k):
        for d in (0, 1):
            zs = source(d, k)

            @pl.when(k <= last(d, 0))
            def _():
                scale_hop(d, zs, k - 1).wait_recv()

            @pl.when(k < last(d, 0))
            def _():
                scale_hop(d, zs, k).start()

    def pair_of(j):
        return (z + nz - j % half) % nz, (z + j) % nz

    def wait_across(p, j):
        for several in (1, 2):

            @pl.when((j < half) == (several == 2))
            def _():
                pieces = w.at[pl.ds(0, several), pl.ds(base[p], alone[p])]
                copy(pieces, pieces, ysend.at[p], yrecv.at[p, j - 1], partner).wait_recv()

    own_rows = pl.ds(pl.multiple_of(t * rows, rows), rows)
    hr = rows // 2

    def chunk(r, tt, h):
        return act.at[r, pl.ds(pl.multiple_of(tt * rows + h * hr, hr), hr)]

    def g_half(r, i, tt, h, device):
        return copy(chunk(r, tt, h), chunk(r, tt, h), gsend.at[r], grecv.at[r, i if i < 7 else 0], device)

    def g_whole(r):
        return copy(act.at[r, own_rows], act.at[r, own_rows], gsend.at[r], grecv.at[r, 0], sibling)

    far = (x + 2) % nx

    def gather_start(r):
        g_half(r, 1, t, 0, right_x).start()
        g_half(r, 4, t, 1, left_x).start()
        g_half(r, 2, t, 1, right_x).start()
        g_half(r, 3, t, 0, left_x).start()
        g_whole(r).start()

    def gather_middle(r):
        from_left, from_right = 2 * xl + c, 2 * xr + c
        g_half(r, 1, from_left, 0, right_x).wait_recv()
        g_half(r, 5, from_left, 0, right_x).start()
        g_half(r, 7, from_left, 0, sibling).start()
        g_half(r, 4, from_right, 1, left_x).wait_recv()
        g_half(r, 6, from_right, 1, left_x).start()
        g_half(r, 10, from_right, 1, sibling).start()
        g_half(r, 2, from_left, 1, right_x).wait_recv()
        g_half(r, 8, from_left, 1, sibling).start()
        g_half(r, 3, from_right, 0, left_x).wait_recv()
        g_half(r, 9, from_right, 0, sibling).start()

    def gather_end(r):
        g_half(r, 5, 2 * far + c, 0, right_x).wait_recv()
        g_half(r, 11, 2 * far + c, 0, sibling).start()
        g_half(r, 6, 2 * far + c, 1, left_x).wait_recv()
        g_half(r, 12, 2 * far + c, 1, sibling).start()
        arrived = act.at[r, pl.ds(0, 4 * rows)]
        copy(arrived, arrived, gsend.at[r], grecv.at[r, 0], sibling).wait_recv()

    def gather_drain(r):
        sent = act.at[r, pl.ds(0, 7 * rows)]
        copy(sent, sent, gsend.at[r], grecv.at[r, 0], sibling).wait_send()

    def normalise(r):
        def squares(i, s):
            v = act[r, pl.ds(pl.multiple_of(i * LANES, LANES), LANES)].astype(F32)
            return s + jnp.sum(v * v, axis=0, keepdims=True)

        s = lax.fori_loop(0, nz, squares, jnp.zeros((1, toks), F32))
        inverse = lax.rsqrt(s / (rows * ntp) + EPS)

        def apply(i, _):
            at = pl.ds(pl.multiple_of(i * LANES, LANES), LANES)
            v = act[r, at].astype(F32)
            xn[at] = (v * inverse * cols[at, r : r + 1]).astype(BF16)
            return 0

        lax.fori_loop(0, nz, apply, 0)

    def project_pair(at, n, j, piece):
        a, b = pair_of(j)
        rhs = jnp.concatenate(
            [xn[pl.ds(pl.multiple_of(q * LANES, LANES), LANES)] for q in (a, b)], axis=0
        )

        def one(i, _):
            here = pl.ds(pl.multiple_of(at + i * piece, 16), piece)
            lhs = jnp.concatenate([w[a, here], w[b, here]], axis=1)
            got = jnp.dot(lhs, rhs, preferred_element_type=F32)
            there = pl.ds(pl.multiple_of(i * piece, 16), piece)
            acc[there] = acc[there] + got
            return 0

        lax.fori_loop(0, n // piece, one, 0)

    def clear(n):
        def one(i, _):
            acc[pl.ds(pl.multiple_of(i * 64, 64), 64)] = jnp.zeros((64, toks), F32)
            return 0

        lax.fori_loop(0, n // 64, one, 0)

    def hidden(b):
        def one(i, _):
            at = pl.ds(pl.multiple_of(i * 64, 64), 64)
            up_at = pl.ds(pl.multiple_of(ff + i * 64, 64), 64)
            scale = cols[pl.ds(pl.multiple_of(hidden_at + i * 64, 64), 64)]
            gate = acc[at] * scale[:, 2 * b : 2 * b + 1]
            up = acc[up_at] * scale[:, 2 * b + 1 : 2 * b + 2]
            hid[at] = (gate / (1.0 + jnp.exp(-gate)) * up).astype(BF16)
            return 0

        lax.fori_loop(0, ff // 64, one, 0)

    def to_sibling(r, zs):
        return copy(sb.at[r, zs], pr.at[r, zs], psend.at[r], precv.at[r, zs], sibling)

    def to_owner(r, zs):
        return copy(
            cb.at[r, zs],
            rr.at[r, x, zs % 2],
            csend.at[r],
            crecv.at[r],
            at_tp(2 * (zs // 4) + c),
        )

    def produce(r, j, lhs, rhs):
        product = contract_rows(lhs, rhs)
        for i, zs in enumerate(pair_of(j)):
            col = jnp.transpose(scl[zs])[:, r : r + 1]
            term = product[i * LANES : (i + 1) * LANES] * col
            mine = (zs // 2) % 2 == c

            @pl.when(mine)
            def _():
                pbuf[zs] = term

            @pl.when(jnp.logical_not(mine))
            def _():
                sb[r, zs] = term.astype(BF16)
                to_sibling(r, zs).start()

    def combine(r, j):
        for zs in pair_of(j):

            @pl.when((zs // 2) % 2 == c)
            def _():
                to_sibling(r, zs).wait_recv()
                both = (pbuf[zs] + pr[r, zs].astype(F32)).astype(BF16)

                @pl.when(zs // 4 == x)
                def _():
                    rr[r, x, zs % 2] = both

                @pl.when(zs // 4 != x)
                def _():
                    cb[r, zs] = both
                    to_owner(r, zs).start()

    def finish(r, factor):
        arrived = cb.at[r, pl.ds(0, 2 * (nx - 1))]
        copy(arrived, arrived, csend.at[r], crecv.at[r], sibling).wait_recv()
        news = []
        for h in (0, 1):
            summed = rr[r, 0, h].astype(F32)
            for xs in range(1, nx):
                summed = summed + rr[r, xs, h].astype(F32)
            at = pl.ds(pl.multiple_of(t * rows + h * LANES, LANES), LANES)
            news.append((act[r, at].astype(F32) + factor * summed).astype(BF16))
        return news

    def next_stream(r, factor):
        for h, new in enumerate(finish(r, factor)):
            act[r + 1, pl.ds(pl.multiple_of(t * rows + h * LANES, LANES), LANES)] = new

    def reduce_drain(r):
        sent = sb.at[r, pl.ds(0, half)]
        copy(sent, sent, psend.at[r], precv.at[r, 0], sibling).wait_send()
        sent = cb.at[r, pl.ds(0, 2 * (nx - 1))]
        copy(sent, sent, csend.at[r], crecv.at[r], sibling).wait_send()

    def down_piece(p, r, j):
        a, b = pair_of(j)
        lhs = jnp.concatenate([w[a, pl.ds(base[p], ff)], w[b, pl.ds(base[p], ff)]], axis=1)
        produce(r, j, lhs, hid[...])

    fetch_stream = pltpu.make_async_copy(stream_ref, act.at[0, own_rows], in_sem.at[0])
    fetch_scale = pltpu.make_async_copy(
        vectors_ref.at[:, pl.ds(scale_at, LANES)], scl.at[z], in_sem.at[1]
    )
    fetches = [
        pltpu.make_async_copy(
            pack_ref.at[pl.ds(base[p], total[p])], w.at[z, pl.ds(base[p], total[p])], in_sem.at[2 + p]
        )
        for p in range(5)
    ]
    fetches[0].start()
    fetch_stream.start()
    fetch_scale.start()
    for p in range(1, 5):
        fetches[p].start()

    barrier = pltpu.get_barrier_semaphore()
    peers = [*around, partner] + [at_tp((t + d) % ntp) for d in range(1, ntp)]
    for device in peers:
        pl.semaphore_signal(barrier, inc=1, device_id=device, device_id_type=MESH)
    pl.semaphore_wait(barrier, len(peers))

    fetches[0].wait()
    start_ring(0)
    fetch_stream.wait()
    gather_start(0)
    fetch_scale.wait()
    for d in (0, 1):
        scale_hop(d, z, 0).start()
    for p in range(1, 5):
        fetches[p].wait()
    clear(2 * ff)

    def turn(i, _):
        at = pl.ds(pl.multiple_of(i * LANES, LANES), LANES)
        cols[at] = jnp.transpose(vectors_ref[:, at])
        return 0

    lax.fori_loop(0, vectors_ref.shape[1] // LANES, turn, 0)
    tick(0, 1)
    gather_middle(0)
    scale_tick(1)
    tick(0, 2)
    gather_end(0)
    normalise(0)

    def first_loop(j, _):
        @pl.when(j + 2 <= half)
        def _():
            tick(0, j + 2)
            scale_tick(j + 1)

        @pl.when(j + 2 == half - 1)
        def _():
            start_ring(1)
            start_ring(2)

        @pl.when(j == half)
        def _():
            tick(1, 1)
            tick(2, 1)

        wait_across(0, j)
        project_pair(base[0], 2 * ff, j, ff // 2)
        return 0

    lax.fori_loop(1, half + 1, first_loop, 0)
    scale_tick(half)
    hidden(0)

    def second_loop(j, _):
        @pl.when(j + 1 <= half)
        def _():
            tick(1, j + 1)
            tick(2, j + 1)

        @pl.when(j + 1 == half - 1)
        def _():
            start_ring(3)
            start_ring(4)

        wait_across(1, j)
        down_piece(1, 0, j)

        @pl.when(j > 1)
        def _():
            combine(0, j - 1)

        return 0

    lax.fori_loop(1, half + 1, second_loop, 0)
    combine(0, half)
    tick(3, 1)
    next_stream(0, 0.5)
    gather_start(1)
    tick(4, 1)
    tick(3, 2)
    gather_middle(1)
    tick(4, 2)
    gather_end(1)
    normalise(1)
    tick(3, 3)
    clear(2 * ch)

    def mixer_loop(j, _):
        wait_across(2, j)
        project_pair(base[2], 2 * ch, j, 2 * ch)
        return 0

    lax.fori_loop(1, half + 1, mixer_loop, 0)
    mixer_cols = cols[mixer_at : mixer_at + ch]
    left[...] = jax.nn.gelu(acc[0:ch] * mixer_cols[:, 0:1])
    right[...] = jax.nn.gelu(acc[ch : 2 * ch] * mixer_cols[:, 1:2])
    st_own[...] = jnp.zeros_like(st_own)
    st_own[0:1] = jnp.sum(right[...], axis=0, keepdims=True)
    st_own[1:2] = jnp.sum(right[...] * right[...], axis=0, keepdims=True)

    def to_peer(d):
        return copy(st_own, st.at[t], tsend.at[0], trecv.at[0], at_tp((t + d) % ntp))

    for d in range(1, ntp):
        to_peer(d).start()
    tick(4, 3)
    st[t] = st_own[...]
    arrived = st.at[pl.ds(0, ntp - 1)]
    copy(arrived, arrived, tsend.at[0], trecv.at[0], sibling).wait_recv()
    sums = st[0]
    for i in range(1, ntp):
        sums = sums + st[i]
    average = sums[0:1] / (ch * ntp)
    inverse = lax.rsqrt(sums[1:2] / (ch * ntp) - average * average + EPS)
    centred = ((right[...] - average) * inverse * mixer_cols[:, 2:3]).astype(BF16)
    target = lax.broadcasted_iota(jnp.int32, (span, span), 0)
    origin = lax.broadcasted_iota(jnp.int32, (span, span), 1)
    masked = jnp.where(origin <= target, spatial_ref[...].astype(F32), 0.0).astype(BF16)
    for n in range(toks // span):
        at = slice(n * span, (n + 1) * span)
        mixed = lax.dot_general(
            centred[:, at], masked, (((1,), (1,)), ((), ())), preferred_element_type=F32
        )
        gated[:, at] = (left[:, at] * (mixed + bias_ref[...])).astype(BF16)

    def mixer_out_loop(j, _):
        a, b = pair_of(j)
        here = pl.ds(base[2] + 2 * ch, ch)
        produce(1, j, jnp.concatenate([w[a, here], w[b, here]], axis=1), gated[...])

        @pl.when(j > 2)
        def _():
            combine(1, j - 2)

        @pl.when(j == half // 2)
        def _():
            tick(3, 4)

        return 0

    lax.fori_loop(1, half + 1, mixer_out_loop, 0)
    tick(4, 4)
    combine(1, half - 1)
    combine(1, half)
    tick(3, 5)
    next_stream(1, 1.0)
    gather_start(2)
    tick(4, 5)
    tick(3, 6)
    gather_middle(2)
    tick(4, 6)
    gather_end(2)
    normalise(2)
    clear(2 * ff)

    def third_loop(j, _):
        @pl.when(j == half - 3)
        def _():
            tick(3, half - 1)
            tick(4, half - 1)

        @pl.when(j == half - 1)
        def _():
            tick(3, half)

        wait_across(3, j)
        project_pair(base[3], 2 * ff, j, ff // 2)
        return 0

    lax.fori_loop(1, half + 1, third_loop, 0)
    tick(4, half)
    hidden(1)

    def fourth_loop(j, _):
        wait_across(4, j)
        down_piece(4, 2, j)

        @pl.when(j > 2)
        def _():
            combine(2, j - 2)

        return 0

    lax.fori_loop(1, half + 1, fourth_loop, 0)
    combine(2, half - 1)
    combine(2, half)
    for h, new in enumerate(finish(2, 0.5)):
        out_ref[h * LANES : (h + 1) * LANES] = new

    for p in range(5):
        sent = w.at[pl.ds(0, nz - 1), pl.ds(base[p], total[p] - alone[p])]
        copy(sent, sent, zsend.at[p], zrecv.at[p, 0, 0, 0], sibling).wait_send()
        sent = w.at[pl.ds(0, nz - 1), pl.ds(base[p], alone[p])]
        copy(sent, sent, ysend.at[p], yrecv.at[p, 0], sibling).wait_send()
    sent = scl.at[pl.ds(0, nz - 1)]
    copy(sent, sent, ssend.at[0], srecv.at[0, 0], sibling).wait_send()
    for r in range(3):
        gather_drain(r)
        reduce_drain(r)
    sent = st.at[pl.ds(0, ntp - 1)]
    copy(sent, sent, tsend.at[0], trecv.at[0], sibling).wait_send()


def solution(mesh):
    nz, ntp = mesh.shape["fs"], mesh.shape["tp"]

    def local(
        stream,
        first_gain,
        first_gate,
        first_gate_scale,
        first_up,
        first_up_scale,
        first_down,
        first_down_scale,
        mixer_gain,
        mixer_left,
        mixer_left_scale,
        mixer_right,
        mixer_right_scale,
        channel_gain,
        spatial,
        spatial_bias,
        mixer_out,
        mixer_out_scale,
        second_gain,
        second_gate,
        second_gate_scale,
        second_up,
        second_up_scale,
        second_down,
        second_down_scale,
    ):
        rows, toks = stream.shape
        width, ff = first_gate.shape
        ch, span = mixer_left.shape[1], spatial.shape[1]
        whole = width * nz
        pack = jnp.concatenate(
            [
                first_gate.T,
                first_up.T,
                first_down,
                mixer_left.T,
                mixer_right.T,
                mixer_out,
                second_gate.T,
                second_up.T,
                second_down,
            ],
            axis=0,
        ).astype(BF16)

        def eight_rows(*vectors):
            return jnp.pad(jnp.stack(vectors), ((0, 8 - len(vectors)), (0, -vectors[0].shape[0] % LANES)))

        vectors = jnp.concatenate(
            [
                eight_rows(first_gain, mixer_gain, second_gain),
                eight_rows(first_gate_scale, first_up_scale, second_gate_scale, second_up_scale),
                eight_rows(mixer_left_scale, mixer_right_scale, channel_gain),
                eight_rows(first_down_scale, mixer_out_scale, second_down_scale),
            ],
            axis=1,
        )
        depth = pack.shape[0]
        dma, half = pltpu.SemaphoreType.DMA, nz // 2
        vmem, anywhere = pl.BlockSpec(memory_space=pltpu.VMEM), pl.BlockSpec(memory_space=pl.ANY)
        sizes = (nz, ntp, ff, ch, span)

        def body(*refs):
            kernel(sizes, *refs)

        piece = (nz, LANES, toks)
        return pl.pallas_call(
            body,
            out_shape=jax.ShapeDtypeStruct((rows, toks), BF16),
            in_specs=[anywhere, anywhere] + [vmem] * 3,
            out_specs=vmem,
            scratch_shapes=[
                pltpu.VMEM((nz, depth, LANES), BF16),
                pltpu.VMEM((nz, 8, LANES), F32),
                pltpu.VMEM((vectors.shape[1], 8), F32),
                pltpu.VMEM((3, whole, toks), BF16),
                pltpu.VMEM((whole, toks), BF16),
                pltpu.VMEM((2 * ff, toks), F32),
                pltpu.VMEM((ff, toks), BF16),
                pltpu.VMEM((ch, toks), BF16),
                pltpu.VMEM((ch, toks), F32),
                pltpu.VMEM((ch, toks), F32),
                pltpu.VMEM(piece, F32),
                pltpu.VMEM((3, *piece), BF16),
                pltpu.VMEM((3, *piece), BF16),
                pltpu.VMEM((3, *piece), BF16),
                pltpu.VMEM((3, ntp // 2, 2, LANES, toks), BF16),
                pltpu.VMEM((ntp, 8, toks), F32),
                pltpu.VMEM((8, toks), F32),
                dma((7,)),
                dma((5,)),
                dma((5, 2, 2, half)),
                dma((1,)),
                dma((2, half)),
                dma((5,)),
                dma((5, half)),
                dma((3,)),
                dma((3, nz)),
                dma((3,)),
                dma((3,)),
                dma((3,)),
                dma((3, 7)),
                dma((1,)),
                dma((1,)),
            ],
            compiler_params=pltpu.CompilerParams(
                collective_id=0, has_side_effects=True, vmem_limit_bytes=60 * 1024 * 1024
            ),
            name="layer",
        )(stream, pack, vectors, spatial.reshape(span, span), spatial_bias)

    return jax.shard_map(
        local,
        mesh=mesh,
        in_specs=(
            P("tp", ("grp", "fs")),
            P(),
            P("fs", "tp"),
            P("tp"),
            P("fs", "tp"),
            P("tp"),
            P("tp", "fs"),
            P("fs"),
            P(),
            P("fs", "tp"),
            P("tp"),
            P("fs", "tp"),
            P("tp"),
            P("tp"),
            P("tp", None, None),
            P("tp", None),
            P("tp", "fs"),
            P("fs"),
            P(),
            P("fs", "tp"),
            P("tp"),
            P("fs", "tp"),
            P("tp"),
            P("tp", "fs"),
            P("fs"),
        ),
        out_specs=P("tp", ("grp", "fs")),
        check_vma=False,
    )
```

```python
import jax
import jax.numpy as jnp
from jax import lax
from jax.experimental import pallas as pl
from jax.experimental.pallas import tpu as pltpu
from jax.sharding import PartitionSpec as P

MESH = pl.DeviceIdType.MESH
EPS = 1e-06
F32, BF16 = jnp.float32, jnp.bfloat16
LANES = 128


def contract_rows(a, b):
    return lax.dot_general(a, b, (((0,), (0,)), ((), ())), preferred_element_type=F32)


def kernel(
    sizes,
    stream_ref,
    pack_ref,
    vectors_ref,
    spatial_ref,
    bias_ref,
    out_ref,
    w,
    scl,
    scol,
    cols,
    act,
    xn,
    acc,
    hid,
    gated,
    left,
    right,
    pbuf,
    sb,
    pr,
    cb,
    rl,
    rr,
    st,
    st_own,
    in_sem,
    zsend,
    zrecv,
    ssend,
    srecv,
    ysend,
    yrecv,
    psend,
    precv,
    csend,
    crecv,
    lrecv,
    gsend,
    grecv,
    tsend,
    trecv,
):
    nz, ntp, ff, ch, span = sizes
    nx, half = ntp // 2, nz // 2
    hidden_at = vectors_ref.shape[1] - 2 * LANES - (-ff % LANES) - ff
    mixer_at = vectors_ref.shape[1] - 2 * LANES
    scale_at = vectors_ref.shape[1] - LANES
    rows, toks = stream_ref.shape
    g, z, t = lax.axis_index("grp"), lax.axis_index("fs"), lax.axis_index("tp")
    x, c = t // 2, t % 2
    gp = g % 2

    def at_tp(other):
        return (g, z, other)

    partner = (g + 1 - 2 * gp, z, t)
    sibling = at_tp(2 * x + 1 - c)
    xr, xl = (x + 1) % nx, (x + nx - 1) % nx
    right_x, left_x = at_tp(2 * xr + c), at_tp(2 * xl + c)
    around = ((g, (z + 1) % nz, t), (g, (z + nz - 1) % nz, t))

    def copy(src, dst, send, recv, device):
        return pltpu.make_async_remote_copy(
            src_ref=src, dst_ref=dst, send_sem=send, recv_sem=recv, device_id=device, device_id_type=MESH
        )

    third = ff * 15 // 44
    alone = (2 * third, third, ch, 2 * third - 32, third - 48)
    total = (2 * ff, ff, 3 * ch, 2 * ff, ff)
    base, first = [], 0
    for n in total:
        base.append(first)
        first += n

    def part(p, sub, zs):
        shared = total[p] - 2 * alone[p]
        if sub == 0:
            return w.at[zs, pl.ds(pl.multiple_of(base[p] + gp * (alone[p] + shared), 16), alone[p])]
        return w.at[zs, pl.ds(base[p] + alone[p], shared)]

    def source(d, k):
        return (z + nz - k) % nz if d == 0 else (z + k) % nz

    def last(d, sub):
        return half if d == sub else half - 1

    def hop(p, d, sub, zs, k):
        return copy(part(p, sub, zs), part(p, sub, zs), zsend.at[p], zrecv.at[p, d, sub, k], around[d])

    def scale_hop(d, zs, k):
        return copy(scl.at[zs], scl.at[zs], ssend.at[0], srecv.at[d, k], around[d])

    def across(p, zs, k):
        return copy(part(p, 0, zs), part(p, 0, zs), ysend.at[p], yrecv.at[p, k - 1], partner)

    def start_ring(p):
        for sub in (0, 1):
            for d in (0, 1):
                hop(p, d, sub, z, 0).start()

    def tick(p, k):
        for sub in (0, 1):
            for d in (0, 1):
                zs = source(d, k)

                @pl.when(k <= last(d, sub))
                def _():
                    hop(p, d, sub, zs, k - 1).wait_recv()

                @pl.when(k < last(d, sub))
                def _():
                    hop(p, d, sub, zs, k).start()

                if sub == 0:

                    @pl.when(k <= last(d, sub))
                    def _():
                        across(p, zs, k).start()

    def scale_tick(k):
        for d in (0, 1):
            zs = source(d, k)

            @pl.when(k <= last(d, 0))
            def _():
                scale_hop(d, zs, k - 1).wait_recv()

            @pl.when(k < last(d, 0))
            def _():
                scale_hop(d, zs, k).start()

    def pair_of(j):
        return (z + nz - j % half) % nz, (z + j) % nz

    def wait_across(p, j):
        for several in (1, 2):

            @pl.when((j < half) == (several == 2))
            def _():
                pieces = w.at[pl.ds(0, several), pl.ds(base[p], alone[p])]
                copy(pieces, pieces, ysend.at[p], yrecv.at[p, j - 1], partner).wait_recv()

    own_rows = pl.ds(pl.multiple_of(t * rows, rows), rows)
    hr = rows // 2

    def chunk(r, tt, h):
        return act.at[r, pl.ds(pl.multiple_of(tt * rows + h * hr, hr), hr)]

    def g_half(r, i, tt, h, device):
        return copy(chunk(r, tt, h), chunk(r, tt, h), gsend.at[r], grecv.at[r, i if i < 7 else 0], device)

    def g_whole(r):
        return copy(act.at[r, own_rows], act.at[r, own_rows], gsend.at[r], grecv.at[r, 0], sibling)

    far = (x + 2) % nx

    def gather_start(r):
        g_half(r, 1, t, 0, right_x).start()
        g_half(r, 4, t, 1, left_x).start()
        g_half(r, 2, t, 1, right_x).start()
        g_half(r, 3, t, 0, left_x).start()
        g_whole(r).start()

    def gather_middle(r):
        from_left, from_right = 2 * xl + c, 2 * xr + c
        g_half(r, 1, from_left, 0, right_x).wait_recv()
        g_half(r, 5, from_left, 0, right_x).start()
        g_half(r, 7, from_left, 0, sibling).start()
        g_half(r, 4, from_right, 1, left_x).wait_recv()
        g_half(r, 6, from_right, 1, left_x).start()
        g_half(r, 10, from_right, 1, sibling).start()
        g_half(r, 2, from_left, 1, right_x).wait_recv()
        g_half(r, 8, from_left, 1, sibling).start()
        g_half(r, 3, from_right, 0, left_x).wait_recv()
        g_half(r, 9, from_right, 0, sibling).start()

    def gather_end(r):
        g_half(r, 5, 2 * far + c, 0, right_x).wait_recv()
        g_half(r, 11, 2 * far + c, 0, sibling).start()
        g_half(r, 6, 2 * far + c, 1, left_x).wait_recv()
        g_half(r, 12, 2 * far + c, 1, sibling).start()
        arrived = act.at[r, pl.ds(0, 4 * rows)]
        copy(arrived, arrived, gsend.at[r], grecv.at[r, 0], sibling).wait_recv()

    def gather_drain(r):
        sent = act.at[r, pl.ds(0, 7 * rows)]
        copy(sent, sent, gsend.at[r], grecv.at[r, 0], sibling).wait_send()

    def normalise(r):
        def squares(i, s):
            v = act[r, pl.ds(pl.multiple_of(i * LANES, LANES), LANES)].astype(F32)
            return s + jnp.sum(v * v, axis=0, keepdims=True)

        s = lax.fori_loop(0, nz, squares, jnp.zeros((1, toks), F32))
        inverse = lax.rsqrt(s / (rows * ntp) + EPS)

        def apply(i, _):
            at = pl.ds(pl.multiple_of(i * LANES, LANES), LANES)
            v = act[r, at].astype(F32)
            xn[at] = (v * inverse * cols[at, r : r + 1]).astype(BF16)
            return 0

        lax.fori_loop(0, nz, apply, 0)

    def project_pair(at, n, j, piece):
        a, b = pair_of(j)
        rhs = jnp.concatenate(
            [xn[pl.ds(pl.multiple_of(q * LANES, LANES), LANES)] for q in (a, b)], axis=0
        )

        def one(i, _):
            here = pl.ds(pl.multiple_of(at + i * piece, 16), piece)
            lhs = jnp.concatenate([w[a, here], w[b, here]], axis=1)
            got = jnp.dot(lhs, rhs, preferred_element_type=F32)
            there = pl.ds(pl.multiple_of(i * piece, 16), piece)
            acc[there] = acc[there] + got
            return 0

        lax.fori_loop(0, n // piece, one, 0)

    def clear(n):
        def one(i, _):
            acc[pl.ds(pl.multiple_of(i * 64, 64), 64)] = jnp.zeros((64, toks), F32)
            return 0

        lax.fori_loop(0, n // 64, one, 0)

    def hidden(b):
        def one(i, _):
            at = pl.ds(pl.multiple_of(i * 64, 64), 64)
            up_at = pl.ds(pl.multiple_of(ff + i * 64, 64), 64)
            scale = cols[pl.ds(pl.multiple_of(hidden_at + i * 64, 64), 64)]
            gate = acc[at] * scale[:, 2 * b : 2 * b + 1]
            up = acc[up_at] * scale[:, 2 * b + 1 : 2 * b + 2]
            hid[at] = (gate / (1.0 + jnp.exp(-gate)) * up).astype(BF16)
            return 0

        lax.fori_loop(0, ff // 64, one, 0)

    def to_sibling(r, zs):
        return copy(sb.at[r, zs], pr.at[r, zs], psend.at[r], precv.at[r, zs], sibling)

    def to_owner(r, zs, slot):
        device = (right_x, left_x, at_tp(2 * far + c))[slot - 1]
        return copy(cb.at[r, zs], rr.at[r, slot, zs % 2], csend.at[r], crecv.at[r], device)

    def to_relay(r, zs, side):
        return copy(cb.at[r, zs], rl.at[r, side], csend.at[r], lrecv.at[r, side], (right_x, left_x)[side])

    def produce(r, pieces, lhs, rhs):
        product = contract_rows(lhs, rhs)
        for i, zs in enumerate(pieces):
            col = scol[zs][:, r : r + 1]
            term = product[i * LANES : (i + 1) * LANES] * col
            mine = (zs // 2) % 2 == c

            @pl.when(mine)
            def _():
                pbuf[zs] = term

            @pl.when(jnp.logical_not(mine))
            def _():
                sb[r, zs] = term.astype(BF16)
                to_sibling(r, zs).start()

    def both_cores(r, zs):
        to_sibling(r, zs).wait_recv()
        return pbuf[zs] + pr[r, zs].astype(F32)

    def combine(r, j):
        for zs in pair_of(j):

            @pl.when((zs // 2) % 2 == c)
            def _():
                both = both_cores(r, zs).astype(BF16)

                @pl.when(zs // 4 == x)
                def _():
                    rr[r, 0, zs % 2] = both

                @pl.when(zs // 4 != x)
                def _():
                    cb[r, zs] = both

                for slot, owner in ((1, xr), (2, xl), (3, far)):

                    @pl.when(zs // 4 == owner)
                    def _():
                        to_owner(r, zs, slot).start()

    def turn_of(i):
        away = jnp.where(i < 2, 2, jnp.where(i < 6, 1 + 2 * (i % 2), 0))
        return away, (x + away) % nx, ((i + 1) // 2) % 2

    def pieces_of(i):
        _, owner, q = turn_of(i)
        return 4 * owner + q, 4 * owner + 2 + q

    def combine_turn(r, i):
        away, owner, q = turn_of(i)
        zs = 4 * owner + 2 * c + q
        both = both_cores(r, zs)

        @pl.when(away == 0)
        def _():
            rr[r, 0, q] = both.astype(BF16)

        for side in (0, 1):

            @pl.when(jnp.logical_and(away == 2, q == side))
            def _():
                cb[r, zs] = both.astype(BF16)
                to_relay(r, zs, side).start()

            @pl.when(jnp.logical_and(away == 1 + 2 * side, q != side))
            def _():
                cb[r, zs] = both.astype(BF16)
                to_owner(r, zs, 1 + side).start()

            @pl.when(jnp.logical_and(away == 1 + 2 * side, q == side))
            def _():
                to_relay(r, zs, side).wait_recv()
                cb[r, zs] = (both + rl[r, side].astype(F32)).astype(BF16)
                to_owner(r, zs, 1 + side).start()

    def finish(r, factor):
        slots = (0, 1, 2, 3) if r == 0 else (0, 1, 2)
        arrived = cb.at[r, pl.ds(0, 2 * len(slots) - 2)]
        copy(arrived, arrived, csend.at[r], crecv.at[r], sibling).wait_recv()
        news = []
        for h in (0, 1):
            summed = rr[r, 0, h].astype(F32)
            for slot in slots[1:]:
                summed = summed + rr[r, slot, h].astype(F32)
            at = pl.ds(pl.multiple_of(t * rows + h * LANES, LANES), LANES)
            news.append((act[r, at].astype(F32) + factor * summed).astype(BF16))
        return news

    def next_stream(r, factor):
        for h, new in enumerate(finish(r, factor)):
            act[r + 1, pl.ds(pl.multiple_of(t * rows + h * LANES, LANES), LANES)] = new

    def reduce_drain(r):
        sent = sb.at[r, pl.ds(0, half)]
        copy(sent, sent, psend.at[r], precv.at[r, 0], sibling).wait_send()
        sent = cb.at[r, pl.ds(0, 2 * (nx - 1))]
        copy(sent, sent, csend.at[r], crecv.at[r], sibling).wait_send()

    def down_piece(p, r, pieces):
        a, b = pieces
        lhs = jnp.concatenate([w[a, pl.ds(base[p], ff)], w[b, pl.ds(base[p], ff)]], axis=1)
        produce(r, pieces, lhs, hid[...])

    fetch_stream = pltpu.make_async_copy(stream_ref, act.at[0, own_rows], in_sem.at[0])
    fetch_scale = pltpu.make_async_copy(
        vectors_ref.at[:, pl.ds(scale_at, LANES)], scl.at[z], in_sem.at[1]
    )
    fetches = [
        pltpu.make_async_copy(
            pack_ref.at[pl.ds(base[p], total[p])], w.at[z, pl.ds(base[p], total[p])], in_sem.at[2 + p]
        )
        for p in range(5)
    ]
    fetches[0].start()
    fetch_stream.start()
    fetch_scale.start()
    for p in range(1, 5):
        fetches[p].start()

    barrier = pltpu.get_barrier_semaphore()
    peers = [*around, partner] + [at_tp((t + d) % ntp) for d in range(1, ntp)]
    for device in peers:
        pl.semaphore_signal(barrier, inc=1, device_id=device, device_id_type=MESH)
    pl.semaphore_wait(barrier, len(peers))

    fetches[0].wait()
    start_ring(0)
    fetch_stream.wait()
    gather_start(0)
    fetch_scale.wait()
    for d in (0, 1):
        scale_hop(d, z, 0).start()
    for p in range(1, 5):
        fetches[p].wait()
    clear(2 * ff)

    def turn(i, _):
        at = pl.ds(pl.multiple_of(i * LANES, LANES), LANES)
        cols[at] = jnp.transpose(vectors_ref[:, at])
        return 0

    lax.fori_loop(0, vectors_ref.shape[1] // LANES, turn, 0)
    tick(0, 1)
    gather_middle(0)
    scale_tick(1)
    tick(0, 2)
    gather_end(0)
    normalise(0)

    def first_loop(j, _):
        @pl.when(j + 2 <= half)
        def _():
            tick(0, j + 2)
            scale_tick(j + 1)

        @pl.when(j + 2 == half - 1)
        def _():
            start_ring(1)
            start_ring(2)

        @pl.when(j == half)
        def _():
            tick(1, 1)
            tick(2, 1)

        wait_across(0, j)
        project_pair(base[0], 2 * ff, j, ff // 2)
        return 0

    lax.fori_loop(1, half + 1, first_loop, 0)
    scale_tick(half)
    hidden(0)

    def turn_scale(q, _):
        scol[q] = jnp.transpose(scl[q])
        return 0

    lax.fori_loop(0, nz, turn_scale, 0)

    def inside(j):
        return jnp.logical_and(j >= 1, j <= half)

    def second_loop(j, _):
        @pl.when(j + 1 <= half)
        def _():
            tick(1, j + 1)
            tick(2, j + 1)

        @pl.when(j + 1 == half - 1)
        def _():
            start_ring(3)
            start_ring(4)

        @pl.when(j <= half)
        def _():
            wait_across(1, j)
            down_piece(1, 0, pair_of(j))

        @pl.when(inside(j - 1))
        def _():
            combine(0, j - 1)

        return 0

    lax.fori_loop(1, half + 2, second_loop, 0)
    tick(3, 1)
    next_stream(0, 0.5)
    gather_start(1)
    tick(4, 1)
    tick(3, 2)
    gather_middle(1)
    tick(4, 2)
    gather_end(1)
    normalise(1)
    tick(3, 3)
    clear(2 * ch)

    def mixer_loop(j, _):
        wait_across(2, j)
        project_pair(base[2], 2 * ch, j, 2 * ch)
        return 0

    lax.fori_loop(1, half + 1, mixer_loop, 0)
    mixer_cols = cols[mixer_at : mixer_at + ch]
    left[...] = jax.nn.gelu(acc[0:ch] * mixer_cols[:, 0:1])
    right[...] = jax.nn.gelu(acc[ch : 2 * ch] * mixer_cols[:, 1:2])
    st_own[...] = jnp.zeros_like(st_own)
    st_own[0:1] = jnp.sum(right[...], axis=0, keepdims=True)
    st_own[1:2] = jnp.sum(right[...] * right[...], axis=0, keepdims=True)

    def to_peer(d):
        return copy(st_own, st.at[t], tsend.at[0], trecv.at[0], at_tp((t + d) % ntp))

    for d in range(1, ntp):
        to_peer(d).start()
    tick(4, 3)
    st[t] = st_own[...]
    arrived = st.at[pl.ds(0, ntp - 1)]
    copy(arrived, arrived, tsend.at[0], trecv.at[0], sibling).wait_recv()
    sums = st[0]
    for i in range(1, ntp):
        sums = sums + st[i]
    average = sums[0:1] / (ch * ntp)
    inverse = lax.rsqrt(sums[1:2] / (ch * ntp) - average * average + EPS)
    centred = ((right[...] - average) * inverse * mixer_cols[:, 2:3]).astype(BF16)
    target = lax.broadcasted_iota(jnp.int32, (span, span), 0)
    origin = lax.broadcasted_iota(jnp.int32, (span, span), 1)
    masked = jnp.where(origin <= target, spatial_ref[...].astype(F32), 0.0).astype(BF16)
    for n in range(toks // span):
        at = slice(n * span, (n + 1) * span)
        mixed = lax.dot_general(
            centred[:, at], masked, (((1,), (1,)), ((), ())), preferred_element_type=F32
        )
        gated[:, at] = (left[:, at] * (mixed + bias_ref[...])).astype(BF16)

    def mixer_out_loop(i, _):
        @pl.when(i < half)
        def _():
            a, b = pieces_of(i)
            here = pl.ds(base[2] + 2 * ch, ch)
            produce(1, (a, b), jnp.concatenate([w[a, here], w[b, here]], axis=1), gated[...])

        @pl.when(i >= 3)
        def _():
            combine_turn(1, i - 3)

        @pl.when(i == 3)
        def _():
            tick(3, 4)

        @pl.when(i == half)
        def _():
            tick(4, 4)

        return 0

    lax.fori_loop(0, half + 3, mixer_out_loop, 0)
    tick(3, 5)
    next_stream(1, 1.0)
    gather_start(2)
    tick(4, 5)
    gather_middle(2)
    tick(3, 6)
    gather_end(2)
    tick(4, 6)
    normalise(2)
    clear(2 * ff)
    tick(3, half - 1)

    def third_loop(j, _):
        @pl.when(j == 2)
        def _():
            tick(4, half - 1)

        @pl.when(j == half - 2)
        def _():
            tick(3, half)

        @pl.when(j == half - 1)
        def _():
            tick(4, half)

        wait_across(3, j)
        project_pair(base[3], 2 * ff, j, ff // 2)
        return 0

    lax.fori_loop(1, half + 1, third_loop, 0)
    hidden(1)

    for j in range(1, half + 1):
        wait_across(4, j)

    def fourth_loop(i, _):
        @pl.when(i < half)
        def _():
            down_piece(4, 2, pieces_of(i))

        @pl.when(i >= 2)
        def _():
            combine_turn(2, i - 2)

        return 0

    lax.fori_loop(0, half + 2, fourth_loop, 0)
    for h, new in enumerate(finish(2, 0.5)):
        out_ref[h * LANES : (h + 1) * LANES] = new

    for p in range(5):
        sent = w.at[pl.ds(0, nz - 1), pl.ds(base[p], total[p] - alone[p])]
        copy(sent, sent, zsend.at[p], zrecv.at[p, 0, 0, 0], sibling).wait_send()
        sent = w.at[pl.ds(0, nz - 1), pl.ds(base[p], alone[p])]
        copy(sent, sent, ysend.at[p], yrecv.at[p, 0], sibling).wait_send()
    sent = scl.at[pl.ds(0, nz - 1)]
    copy(sent, sent, ssend.at[0], srecv.at[0, 0], sibling).wait_send()
    for r in range(3):
        gather_drain(r)
        reduce_drain(r)
    sent = st.at[pl.ds(0, ntp - 1)]
    copy(sent, sent, tsend.at[0], trecv.at[0], sibling).wait_send()


def solution(mesh):
    nz, ntp = mesh.shape["fs"], mesh.shape["tp"]

    def local(
        stream,
        first_gain,
        first_gate,
        first_gate_scale,
        first_up,
        first_up_scale,
        first_down,
        first_down_scale,
        mixer_gain,
        mixer_left,
        mixer_left_scale,
        mixer_right,
        mixer_right_scale,
        channel_gain,
        spatial,
        spatial_bias,
        mixer_out,
        mixer_out_scale,
        second_gain,
        second_gate,
        second_gate_scale,
        second_up,
        second_up_scale,
        second_down,
        second_down_scale,
    ):
        rows, toks = stream.shape
        width, ff = first_gate.shape
        ch, span = mixer_left.shape[1], spatial.shape[1]
        whole = width * nz
        pack = jnp.concatenate(
            [
                first_gate.T,
                first_up.T,
                first_down,
                mixer_left.T,
                mixer_right.T,
                mixer_out,
                second_gate.T,
                second_up.T,
                second_down,
            ],
            axis=0,
        ).astype(BF16)

        def eight_rows(*vectors):
            return jnp.pad(jnp.stack(vectors), ((0, 8 - len(vectors)), (0, -vectors[0].shape[0] % LANES)))

        vectors = jnp.concatenate(
            [
                eight_rows(first_gain, mixer_gain, second_gain),
                eight_rows(first_gate_scale, first_up_scale, second_gate_scale, second_up_scale),
                eight_rows(mixer_left_scale, mixer_right_scale, channel_gain),
                eight_rows(first_down_scale, mixer_out_scale, second_down_scale),
            ],
            axis=1,
        )
        depth = pack.shape[0]
        dma, half = pltpu.SemaphoreType.DMA, nz // 2
        vmem, anywhere = pl.BlockSpec(memory_space=pltpu.VMEM), pl.BlockSpec(memory_space=pl.ANY)
        sizes = (nz, ntp, ff, ch, span)

        def body(*refs):
            kernel(sizes, *refs)

        piece = (nz, LANES, toks)
        return pl.pallas_call(
            body,
            out_shape=jax.ShapeDtypeStruct((rows, toks), BF16),
            in_specs=[anywhere, anywhere] + [vmem] * 3,
            out_specs=vmem,
            scratch_shapes=[
                pltpu.VMEM((nz, depth, LANES), BF16),
                pltpu.VMEM((nz, 8, LANES), F32),
                pltpu.VMEM((nz, LANES, 8), F32),
                pltpu.VMEM((vectors.shape[1], 8), F32),
                pltpu.VMEM((3, whole, toks), BF16),
                pltpu.VMEM((whole, toks), BF16),
                pltpu.VMEM((2 * ff, toks), F32),
                pltpu.VMEM((ff, toks), BF16),
                pltpu.VMEM((ch, toks), BF16),
                pltpu.VMEM((ch, toks), F32),
                pltpu.VMEM((ch, toks), F32),
                pltpu.VMEM(piece, F32),
                pltpu.VMEM((3, *piece), BF16),
                pltpu.VMEM((3, *piece), BF16),
                pltpu.VMEM((3, *piece), BF16),
                pltpu.VMEM((3, 2, LANES, toks), BF16),
                pltpu.VMEM((3, 4, 2, LANES, toks), BF16),
                pltpu.VMEM((ntp, 8, toks), F32),
                pltpu.VMEM((8, toks), F32),
                dma((7,)),
                dma((5,)),
                dma((5, 2, 2, half)),
                dma((1,)),
                dma((2, half)),
                dma((5,)),
                dma((5, half)),
                dma((3,)),
                dma((3, nz)),
                dma((3,)),
                dma((3,)),
                dma((3, 2)),
                dma((3,)),
                dma((3, 7)),
                dma((1,)),
                dma((1,)),
            ],
            compiler_params=pltpu.CompilerParams(
                collective_id=0, has_side_effects=True, vmem_limit_bytes=60 * 1024 * 1024
            ),
            name="layer",
        )(stream, pack, vectors, spatial.reshape(span, span), spatial_bias)

    return jax.shard_map(
        local,
        mesh=mesh,
        in_specs=(
            P("tp", ("grp", "fs")),
            P(),
            P("fs", "tp"),
            P("tp"),
            P("fs", "tp"),
            P("tp"),
            P("tp", "fs"),
            P("fs"),
            P(),
            P("fs", "tp"),
            P("tp"),
            P("fs", "tp"),
            P("tp"),
            P("tp"),
            P("tp", None, None),
            P("tp", None),
            P("tp", "fs"),
            P("fs"),
            P(),
            P("fs", "tp"),
            P("tp"),
            P("fs", "tp"),
            P("tp"),
            P("tp", "fs"),
            P("fs"),
        ),
        out_specs=P("tp", ("grp", "fs")),
        check_vma=False,
    )
```

```python
import jax
import jax.numpy as jnp
from jax import lax
from jax.experimental import pallas as pl
from jax.experimental.pallas import tpu as pltpu
from jax.sharding import PartitionSpec as P

MESH = pl.DeviceIdType.MESH
EPS = 1e-06
F32, BF16 = jnp.float32, jnp.bfloat16
LANES = 128


def contract_rows(a, b):
    return lax.dot_general(a, b, (((0,), (0,)), ((), ())), preferred_element_type=F32)


def kernel(
    sizes,
    stream_ref,
    first_gate_ref,
    first_up_ref,
    first_down_ref,
    left_ref,
    right_ref,
    mixer_out_ref,
    second_gate_ref,
    second_up_ref,
    second_down_ref,
    vectors_ref,
    spatial_ref,
    bias_ref,
    out_ref,
    wide,
    tall,
    small,
    w,
    scl,
    scol,
    cols,
    act,
    xn,
    acc,
    hid,
    gated,
    left,
    right,
    pbuf,
    sb,
    pr,
    cb,
    rl,
    rr,
    st,
    st_own,
    in_sem,
    zsend,
    zrecv,
    ssend,
    srecv,
    ysend,
    yrecv,
    psend,
    precv,
    csend,
    crecv,
    lrecv,
    gsend,
    grecv,
    tsend,
    trecv,
):
    nz, ntp, ff, ch, span = sizes
    nx, half = ntp // 2, nz // 2
    hidden_at = vectors_ref.shape[1] - 2 * LANES - (-ff % LANES) - ff
    mixer_at = vectors_ref.shape[1] - 2 * LANES
    scale_at = vectors_ref.shape[1] - LANES
    rows, toks = stream_ref.shape
    g, z, t = lax.axis_index("grp"), lax.axis_index("fs"), lax.axis_index("tp")
    x, c = t // 2, t % 2
    gp = g % 2

    def at_tp(other):
        return (g, z, other)

    partner = (g + 1 - 2 * gp, z, t)
    sibling = at_tp(2 * x + 1 - c)
    xr, xl = (x + 1) % nx, (x + nx - 1) % nx
    right_x, left_x = at_tp(2 * xr + c), at_tp(2 * xl + c)
    around = ((g, (z + 1) % nz, t), (g, (z + nz - 1) % nz, t))

    def copy(src, dst, send, recv, device):
        return pltpu.make_async_remote_copy(
            src_ref=src, dst_ref=dst, send_sem=send, recv_sem=recv, device_id=device, device_id_type=MESH
        )

    third = ff * 15 // 44
    alone = (2 * third, third, ch, 2 * third - 32, third - 48)
    total = (2 * ff, ff, 3 * ch, 2 * ff, ff)
    base, first = [], 0
    for n in total:
        base.append(first)
        first += n

    y_slot = (0, 1, 2, 0, 3)

    def part(p, sub, zs):
        shared = total[p] - 2 * alone[p]
        if sub == 0:
            return w.at[zs, pl.ds(pl.multiple_of(base[p] + gp * (alone[p] + shared), 16), alone[p])]
        return w.at[zs, pl.ds(base[p] + alone[p], shared)]

    def source(d, k):
        return (z + nz - k) % nz if d == 0 else (z + k) % nz

    def last(d, sub):
        return half if d == sub else half - 1

    def hop(p, d, sub, zs, k):
        return copy(part(p, sub, zs), part(p, sub, zs), zsend.at[p], zrecv.at[p % 3, d, sub, k], around[d])

    def scale_hop(d, zs, k):
        return copy(scl.at[zs], scl.at[zs], ssend.at[0], srecv.at[d, k], around[d])

    def across(p, zs, k):
        return copy(part(p, 0, zs), part(p, 0, zs), ysend.at[p], yrecv.at[y_slot[p], k - 1], partner)

    def start_ring(p):
        for sub in (0, 1):
            for d in (0, 1):
                hop(p, d, sub, z, 0).start()

    def tick(p, k):
        for sub in (0, 1):
            for d in (0, 1):
                zs = source(d, k)

                @pl.when(k <= last(d, sub))
                def _():
                    hop(p, d, sub, zs, k - 1).wait_recv()

                @pl.when(k < last(d, sub))
                def _():
                    hop(p, d, sub, zs, k).start()

                if sub == 0:

                    @pl.when(k <= last(d, sub))
                    def _():
                        across(p, zs, k).start()

    def scale_tick(k):
        for d in (0, 1):
            zs = source(d, k)

            @pl.when(k <= last(d, 0))
            def _():
                scale_hop(d, zs, k - 1).wait_recv()

            @pl.when(k < last(d, 0))
            def _():
                scale_hop(d, zs, k).start()

    def pair_of(j):
        return (z + nz - j % half) % nz, (z + j) % nz

    def wait_across(p, j):
        for several in (1, 2):

            @pl.when((j < half) == (several == 2))
            def _():
                pieces = w.at[pl.ds(0, several), pl.ds(base[p], alone[p])]
                copy(pieces, pieces, ysend.at[p], yrecv.at[y_slot[p], j - 1], partner).wait_recv()

    own_rows = pl.ds(pl.multiple_of(t * rows, rows), rows)
    hr = rows // 2

    def chunk(r, tt, h):
        return act.at[r, pl.ds(pl.multiple_of(tt * rows + h * hr, hr), hr)]

    def g_half(r, i, tt, h, device):
        return copy(chunk(r, tt, h), chunk(r, tt, h), gsend.at[r], grecv.at[i if i < 7 else 0], device)

    def g_whole(r):
        return copy(act.at[r, own_rows], act.at[r, own_rows], gsend.at[r], grecv.at[0], sibling)

    far = (x + 2) % nx

    def gather_start(r):
        g_half(r, 1, t, 0, right_x).start()
        g_half(r, 4, t, 1, left_x).start()
        g_half(r, 2, t, 1, right_x).start()
        g_half(r, 3, t, 0, left_x).start()
        g_whole(r).start()

    def gather_middle(r):
        from_left, from_right = 2 * xl + c, 2 * xr + c
        g_half(r, 1, from_left, 0, right_x).wait_recv()
        g_half(r, 5, from_left, 0, right_x).start()
        g_half(r, 7, from_left, 0, sibling).start()
        g_half(r, 4, from_right, 1, left_x).wait_recv()
        g_half(r, 6, from_right, 1, left_x).start()
        g_half(r, 10, from_right, 1, sibling).start()
        g_half(r, 2, from_left, 1, right_x).wait_recv()
        g_half(r, 8, from_left, 1, sibling).start()
        g_half(r, 3, from_right, 0, left_x).wait_recv()
        g_half(r, 9, from_right, 0, sibling).start()

    def gather_end(r):
        g_half(r, 5, 2 * far + c, 0, right_x).wait_recv()
        g_half(r, 11, 2 * far + c, 0, sibling).start()
        g_half(r, 6, 2 * far + c, 1, left_x).wait_recv()
        g_half(r, 12, 2 * far + c, 1, sibling).start()
        arrived = act.at[r, pl.ds(0, 4 * rows)]
        copy(arrived, arrived, gsend.at[r], grecv.at[0], sibling).wait_recv()

    def gather_drain(r):
        sent = act.at[r, pl.ds(0, 7 * rows)]
        copy(sent, sent, gsend.at[r], grecv.at[0], sibling).wait_send()

    def normalise(r):
        def squares(i, s):
            v = act[r, pl.ds(pl.multiple_of(i * LANES, LANES), LANES)].astype(F32)
            return s + jnp.sum(v * v, axis=0, keepdims=True)

        s = lax.fori_loop(0, nz, squares, jnp.zeros((1, toks), F32))
        inverse = lax.rsqrt(s / (rows * ntp) + EPS)

        def apply(i, _):
            at = pl.ds(pl.multiple_of(i * LANES, LANES), LANES)
            v = act[r, at].astype(F32)
            xn[at] = (v * inverse * cols[at, r : r + 1]).astype(BF16)
            return 0

        lax.fori_loop(0, nz, apply, 0)

    def project_pair(at, n, j, piece):
        a, b = pair_of(j)
        rhs = jnp.concatenate(
            [xn[pl.ds(pl.multiple_of(q * LANES, LANES), LANES)] for q in (a, b)], axis=0
        )

        def one(i, _):
            here = pl.ds(pl.multiple_of(at + i * piece, 16), piece)
            lhs = jnp.concatenate([w[a, here], w[b, here]], axis=1)
            got = jnp.dot(lhs, rhs, preferred_element_type=F32)
            there = pl.ds(pl.multiple_of(i * piece, 16), piece)
            acc[there] = acc[there] + got
            return 0

        lax.fori_loop(0, n // piece, one, 0)

    def clear(n):
        def one(i, _):
            acc[pl.ds(pl.multiple_of(i * 64, 64), 64)] = jnp.zeros((64, toks), F32)
            return 0

        lax.fori_loop(0, n // 64, one, 0)

    def hidden(b):
        def one(i, _):
            at = pl.ds(pl.multiple_of(i * 64, 64), 64)
            up_at = pl.ds(pl.multiple_of(ff + i * 64, 64), 64)
            scale = cols[pl.ds(pl.multiple_of(hidden_at + i * 64, 64), 64)]
            gate = acc[at] * scale[:, 2 * b : 2 * b + 1]
            up = acc[up_at] * scale[:, 2 * b + 1 : 2 * b + 2]
            hid[at] = (gate / (1.0 + jnp.exp(-gate)) * up).astype(BF16)
            return 0

        lax.fori_loop(0, ff // 64, one, 0)

    def to_sibling(r, zs):
        return copy(sb.at[r, zs], pr.at[r, zs], psend.at[r], precv.at[zs], sibling)

    def to_owner(r, zs, slot):
        device = (right_x, left_x, at_tp(2 * far + c))[slot - 1]
        return copy(cb.at[r, zs], rr.at[r, slot, zs % 2], csend.at[r], crecv.at[r], device)

    def to_relay(r, zs, side):
        return copy(cb.at[r, zs], rl.at[r, side], csend.at[r], lrecv.at[r, side], (right_x, left_x)[side])

    def produce(r, pieces, lhs, rhs):
        product = contract_rows(lhs, rhs)
        for i, zs in enumerate(pieces):
            col = scol[zs][:, r : r + 1]
            term = product[i * LANES : (i + 1) * LANES] * col
            mine = (zs // 2) % 2 == c

            @pl.when(mine)
            def _():
                pbuf[zs] = term

            @pl.when(jnp.logical_not(mine))
            def _():
                sb[r, zs] = term.astype(BF16)
                to_sibling(r, zs).start()

    def both_cores(r, zs):
        to_sibling(r, zs).wait_recv()
        return pbuf[zs] + pr[r, zs].astype(F32)

    def combine(r, j):
        for zs in pair_of(j):

            @pl.when((zs // 2) % 2 == c)
            def _():
                both = both_cores(r, zs).astype(BF16)

                @pl.when(zs // 4 == x)
                def _():
                    rr[r, 0, zs % 2] = both

                @pl.when(zs // 4 != x)
                def _():
                    cb[r, zs] = both

                for slot, owner in ((1, xr), (2, xl), (3, far)):

                    @pl.when(zs // 4 == owner)
                    def _():
                        to_owner(r, zs, slot).start()

    def turn_of(i):
        away = jnp.where(i < 2, 2, jnp.where(i // 2 == 2, 0, 1 + 2 * (i % 2)))
        return away, (x + away) % nx, jnp.where(i < 6, ((i + 1) // 2) % 2, i % 2)

    def pieces_of(i):
        _, owner, q = turn_of(i)
        return 4 * owner + q, 4 * owner + 2 + q

    def combine_turn(r, i):
        away, owner, q = turn_of(i)
        zs = 4 * owner + 2 * c + q
        both = both_cores(r, zs)

        @pl.when(away == 0)
        def _():
            rr[r, 0, q] = both.astype(BF16)

        for side in (0, 1):

            @pl.when(jnp.logical_and(away == 2, q == side))
            def _():
                cb[r, zs] = both.astype(BF16)
                to_relay(r, zs, side).start()

            @pl.when(jnp.logical_and(away == 1 + 2 * side, q != side))
            def _():
                cb[r, zs] = both.astype(BF16)
                to_owner(r, zs, 1 + side).start()

            @pl.when(jnp.logical_and(away == 1 + 2 * side, q == side))
            def _():
                to_relay(r, zs, side).wait_recv()
                cb[r, zs] = (both + rl[r, side].astype(F32)).astype(BF16)
                to_owner(r, zs, 1 + side).start()

    def finish(r, factor):
        slots = (0, 1, 2, 3) if r == 0 else (0, 1, 2)
        arrived = cb.at[r, pl.ds(0, 2 * len(slots) - 2)]
        copy(arrived, arrived, csend.at[r], crecv.at[r], sibling).wait_recv()
        news = []
        for h in (0, 1):
            summed = rr[r, 0, h].astype(F32)
            for slot in slots[1:]:
                summed = summed + rr[r, slot, h].astype(F32)
            at = pl.ds(pl.multiple_of(t * rows + h * LANES, LANES), LANES)
            news.append((act[r, at].astype(F32) + factor * summed).astype(BF16))
        return news

    def next_stream(r, factor):
        for h, new in enumerate(finish(r, factor)):
            act[r + 1, pl.ds(pl.multiple_of(t * rows + h * LANES, LANES), LANES)] = new

    def reduce_drain(r):
        sent = sb.at[r, pl.ds(0, half)]
        copy(sent, sent, psend.at[r], precv.at[0], sibling).wait_send()
        sent = cb.at[r, pl.ds(0, 2 * (nx - 1))]
        copy(sent, sent, csend.at[r], crecv.at[r], sibling).wait_send()

    def down_piece(p, r, pieces):
        a, b = pieces
        lhs = jnp.concatenate([w[a, pl.ds(base[p], ff)], w[b, pl.ds(base[p], ff)]], axis=1)
        produce(r, pieces, lhs, hid[...])

    fetch_stream = pltpu.make_async_copy(stream_ref, act.at[0, own_rows], in_sem.at[0])
    fetch_scale = pltpu.make_async_copy(
        vectors_ref.at[:, pl.ds(scale_at, LANES)], scl.at[z], in_sem.at[1]
    )
    shares = (
        (first_gate_ref, wide.at[0], base[0], True),
        (first_up_ref, wide.at[1], base[0] + ff, True),
        (first_down_ref, tall.at[0], base[1], False),
        (left_ref, small.at[0], base[2], True),
        (right_ref, small.at[1], base[2] + ch, True),
        (mixer_out_ref, small.at[2], base[2] + 2 * ch, False),
        (second_gate_ref, wide.at[2], base[3], True),
        (second_up_ref, wide.at[3], base[3] + ff, True),
        (second_down_ref, tall.at[1], base[4], False),
    )
    fetches = [
        pltpu.make_async_copy(src, held, in_sem.at[2 + i]) for i, (src, held, _, _) in enumerate(shares)
    ]

    def catch(i):
        fetches[i].wait()
        _, held, at, turned = shares[i]
        if not turned:
            w[z, at : at + held.shape[0]] = held[...].astype(BF16)
            return
        for n in range(0, held.shape[1], LANES):
            wid = min(LANES, held.shape[1] - n)
            w[z, at + n : at + n + wid] = jnp.transpose(held[:, n : n + wid]).astype(BF16)

    fetches[0].start()
    fetches[1].start()
    fetch_stream.start()
    fetch_scale.start()
    for fetch in fetches[2:]:
        fetch.start()

    barrier = pltpu.get_barrier_semaphore()
    peers = [*around, partner] + [at_tp((t + d) % ntp) for d in range(1, ntp)]
    for device in peers:
        pl.semaphore_signal(barrier, inc=1, device_id=device, device_id_type=MESH)
    catch(0)
    catch(1)
    pl.semaphore_wait(barrier, len(peers))

    start_ring(0)
    fetch_stream.wait()
    gather_start(0)
    fetch_scale.wait()
    for d in (0, 1):
        scale_hop(d, z, 0).start()
    for i in range(2, 9):
        catch(i)
    clear(2 * ff)

    def turn(i, _):
        at = pl.ds(pl.multiple_of(i * LANES, LANES), LANES)
        cols[at] = jnp.transpose(vectors_ref[:, at])
        return 0

    lax.fori_loop(0, vectors_ref.shape[1] // LANES, turn, 0)
    tick(0, 1)
    gather_middle(0)
    scale_tick(1)
    tick(0, 2)
    gather_end(0)
    normalise(0)

    def first_loop(j, _):
        @pl.when(j + 2 <= half)
        def _():
            tick(0, j + 2)
            scale_tick(j + 1)

        @pl.when(j + 2 == half - 1)
        def _():
            start_ring(1)
            start_ring(2)

        @pl.when(j == half)
        def _():
            tick(1, 1)
            tick(2, 1)

        wait_across(0, j)
        project_pair(base[0], 2 * ff, j, ff // 2)
        return 0

    lax.fori_loop(1, half + 1, first_loop, 0)
    scale_tick(half)
    hidden(0)

    def turn_scale(q, _):
        scol[q] = jnp.transpose(scl[q])
        return 0

    lax.fori_loop(0, nz, turn_scale, 0)

    def inside(j):
        return jnp.logical_and(j >= 1, j <= half)

    def second_loop(j, _):
        @pl.when(j + 1 <= half)
        def _():
            tick(1, j + 1)
            tick(2, j + 1)

        @pl.when(j + 1 == half - 1)
        def _():
            start_ring(3)
            start_ring(4)

        @pl.when(j <= half)
        def _():
            wait_across(1, j)
            down_piece(1, 0, pair_of(j))

        @pl.when(inside(j - 1))
        def _():
            combine(0, j - 1)

        return 0

    lax.fori_loop(1, half + 2, second_loop, 0)
    tick(3, 1)
    next_stream(0, 0.5)
    gather_start(1)
    tick(4, 1)
    tick(3, 2)
    gather_middle(1)
    tick(4, 2)
    gather_end(1)
    normalise(1)
    tick(3, 3)
    clear(2 * ch)

    def mixer_loop(j, _):
        wait_across(2, j)
        project_pair(base[2], 2 * ch, j, 2 * ch)
        return 0

    lax.fori_loop(1, half + 1, mixer_loop, 0)
    mixer_cols = cols[mixer_at : mixer_at + ch]
    left[...] = jax.nn.gelu(acc[0:ch] * mixer_cols[:, 0:1])
    right[...] = jax.nn.gelu(acc[ch : 2 * ch] * mixer_cols[:, 1:2])
    st_own[...] = jnp.zeros_like(st_own)
    st_own[0:1] = jnp.sum(right[...], axis=0, keepdims=True)
    st_own[1:2] = jnp.sum(right[...] * right[...], axis=0, keepdims=True)

    def to_peer(d):
        return copy(st_own, st.at[t], tsend.at[0], trecv.at[0], at_tp((t + d) % ntp))

    for d in range(1, ntp):
        to_peer(d).start()
    tick(4, 3)
    st[t] = st_own[...]
    arrived = st.at[pl.ds(0, ntp - 1)]
    copy(arrived, arrived, tsend.at[0], trecv.at[0], sibling).wait_recv()
    sums = st[0]
    for i in range(1, ntp):
        sums = sums + st[i]
    average = sums[0:1] / (ch * ntp)
    inverse = lax.rsqrt(sums[1:2] / (ch * ntp) - average * average + EPS)
    centred = ((right[...] - average) * inverse * mixer_cols[:, 2:3]).astype(BF16)
    target = lax.broadcasted_iota(jnp.int32, (span, span), 0)
    origin = lax.broadcasted_iota(jnp.int32, (span, span), 1)
    masked = jnp.where(origin <= target, spatial_ref[...].astype(F32), 0.0).astype(BF16)
    for n in range(toks // span):
        at = slice(n * span, (n + 1) * span)
        mixed = lax.dot_general(
            centred[:, at], masked, (((1,), (1,)), ((), ())), preferred_element_type=F32
        )
        gated[:, at] = (left[:, at] * (mixed + bias_ref[...])).astype(BF16)

    def mixer_out_loop(i, _):
        @pl.when(i < half)
        def _():
            a, b = pieces_of(i)
            here = pl.ds(base[2] + 2 * ch, ch)
            produce(1, (a, b), jnp.concatenate([w[a, here], w[b, here]], axis=1), gated[...])

        @pl.when(i >= 3)
        def _():
            combine_turn(1, i - 3)

        @pl.when(i == 3)
        def _():
            tick(3, 4)

        @pl.when(i == half)
        def _():
            tick(4, 4)

        return 0

    lax.fori_loop(0, half + 3, mixer_out_loop, 0)
    tick(3, 5)
    next_stream(1, 1.0)
    gather_start(2)
    tick(4, 5)
    gather_middle(2)
    tick(3, 6)
    gather_end(2)
    normalise(2)
    clear(2 * ff)

    def third_loop(j, _):
        @pl.when(j == 2)
        def _():
            tick(3, half - 1)
            tick(4, half - 2)

        @pl.when(j == half - 3)
        def _():
            tick(3, half)

        @pl.when(j == half - 1)
        def _():
            tick(4, half - 1)

        wait_across(3, j)
        project_pair(base[3], 2 * ff, j, ff // 2)
        return 0

    lax.fori_loop(1, half + 1, third_loop, 0)
    tick(4, half)
    hidden(1)

    for j in range(1, half + 1):
        wait_across(4, j)

    def fourth_loop(i, _):
        @pl.when(i < half)
        def _():
            down_piece(4, 2, pieces_of(i))

        @pl.when(i >= 2)
        def _():
            combine_turn(2, i - 2)

        return 0

    lax.fori_loop(0, half + 2, fourth_loop, 0)
    for h, new in enumerate(finish(2, 0.5)):
        out_ref[h * LANES : (h + 1) * LANES] = new

    for p in range(5):
        sent = w.at[pl.ds(0, nz - 1), pl.ds(base[p], total[p] - alone[p])]
        copy(sent, sent, zsend.at[p], zrecv.at[0, 0, 0, 0], sibling).wait_send()
        sent = w.at[pl.ds(0, nz - 1), pl.ds(base[p], alone[p])]
        copy(sent, sent, ysend.at[p], yrecv.at[0, 0], sibling).wait_send()
    sent = scl.at[pl.ds(0, nz - 1)]
    copy(sent, sent, ssend.at[0], srecv.at[0, 0], sibling).wait_send()
    for r in range(3):
        gather_drain(r)
        reduce_drain(r)
    sent = st.at[pl.ds(0, ntp - 1)]
    copy(sent, sent, tsend.at[0], trecv.at[0], sibling).wait_send()


def solution(mesh):
    nz, ntp = mesh.shape["fs"], mesh.shape["tp"]

    def local(
        stream,
        first_gain,
        first_gate,
        first_gate_scale,
        first_up,
        first_up_scale,
        first_down,
        first_down_scale,
        mixer_gain,
        mixer_left,
        mixer_left_scale,
        mixer_right,
        mixer_right_scale,
        channel_gain,
        spatial,
        spatial_bias,
        mixer_out,
        mixer_out_scale,
        second_gain,
        second_gate,
        second_gate_scale,
        second_up,
        second_up_scale,
        second_down,
        second_down_scale,
    ):
        rows, toks = stream.shape
        width, ff = first_gate.shape
        ch, span = mixer_left.shape[1], spatial.shape[1]
        whole = width * nz
        def eight_rows(*vectors):
            return jnp.pad(jnp.stack(vectors), ((0, 8 - len(vectors)), (0, -vectors[0].shape[0] % LANES)))

        vectors = jnp.concatenate(
            [
                eight_rows(first_gain, mixer_gain, second_gain),
                eight_rows(first_gate_scale, first_up_scale, second_gate_scale, second_up_scale),
                eight_rows(mixer_left_scale, mixer_right_scale, channel_gain),
                eight_rows(first_down_scale, mixer_out_scale, second_down_scale),
            ],
            axis=1,
        )
        depth = 6 * ff + 3 * ch
        dma, half = pltpu.SemaphoreType.DMA, nz // 2
        vmem, anywhere = pl.BlockSpec(memory_space=pltpu.VMEM), pl.BlockSpec(memory_space=pl.ANY)
        sizes = (nz, ntp, ff, ch, span)

        def body(*refs):
            kernel(sizes, *refs)

        piece = (nz, LANES, toks)
        return pl.pallas_call(
            body,
            out_shape=jax.ShapeDtypeStruct((rows, toks), BF16),
            in_specs=[anywhere] * 10 + [vmem] * 3,
            out_specs=vmem,
            scratch_shapes=[
                pltpu.VMEM((4, width, ff), F32),
                pltpu.VMEM((2, ff, width), F32),
                pltpu.VMEM((3, width, ch), F32),
                pltpu.VMEM((nz, depth, LANES), BF16),
                pltpu.VMEM((nz, 8, LANES), F32),
                pltpu.VMEM((nz, LANES, 8), F32),
                pltpu.VMEM((vectors.shape[1], 8), F32),
                pltpu.VMEM((3, whole, toks), BF16),
                pltpu.VMEM((whole, toks), BF16),
                pltpu.VMEM((2 * ff, toks), F32),
                pltpu.VMEM((ff, toks), BF16),
                pltpu.VMEM((ch, toks), BF16),
                pltpu.VMEM((ch, toks), F32),
                pltpu.VMEM((ch, toks), F32),
                pltpu.VMEM(piece, F32),
                pltpu.VMEM((3, *piece), BF16),
                pltpu.VMEM((3, *piece), BF16),
                pltpu.VMEM((3, *piece), BF16),
                pltpu.VMEM((3, 2, LANES, toks), BF16),
                pltpu.VMEM((3, 4, 2, LANES, toks), BF16),
                pltpu.VMEM((ntp, 8, toks), F32),
                pltpu.VMEM((8, toks), F32),
                dma((11,)),
                dma((5,)),
                dma((3, 2, 2, half)),
                dma((1,)),
                dma((2, half)),
                dma((5,)),
                dma((4, half)),
                dma((3,)),
                dma((nz,)),
                dma((3,)),
                dma((3,)),
                dma((3, 2)),
                dma((3,)),
                dma((7,)),
                dma((1,)),
                dma((1,)),
            ],
            compiler_params=pltpu.CompilerParams(
                collective_id=0, has_side_effects=True, vmem_limit_bytes=60 * 1024 * 1024
            ),
            name="layer",
        )(
            stream,
            first_gate,
            first_up,
            first_down,
            mixer_left,
            mixer_right,
            mixer_out,
            second_gate,
            second_up,
            second_down,
            vectors,
            spatial.reshape(span, span),
            spatial_bias,
        )

    return jax.shard_map(
        local,
        mesh=mesh,
        in_specs=(
            P("tp", ("grp", "fs")),
            P(),
            P("fs", "tp"),
            P("tp"),
            P("fs", "tp"),
            P("tp"),
            P("tp", "fs"),
            P("fs"),
            P(),
            P("fs", "tp"),
            P("tp"),
            P("fs", "tp"),
            P("tp"),
            P("tp"),
            P("tp", None, None),
            P("tp", None),
            P("tp", "fs"),
            P("fs"),
            P(),
            P("fs", "tp"),
            P("tp"),
            P("fs", "tp"),
            P("tp"),
            P("tp", "fs"),
            P("fs"),
        ),
        out_specs=P("tp", ("grp", "fs")),
        check_vma=False,
    )
```

```python
import jax
import jax.numpy as jnp
from jax import lax
from jax.experimental import pallas as pl
from jax.experimental.pallas import tpu as pltpu
from jax.sharding import PartitionSpec as P

MESH = pl.DeviceIdType.MESH
EPS = 1e-06
F32, BF16 = jnp.float32, jnp.bfloat16
LANES = 128


def contract_rows(a, b):
    return lax.dot_general(a, b, (((0,), (0,)), ((), ())), preferred_element_type=F32)


def kernel(
    sizes,
    stream_ref,
    first_gate_ref,
    first_up_ref,
    first_down_ref,
    left_ref,
    right_ref,
    mixer_out_ref,
    second_gate_ref,
    second_up_ref,
    second_down_ref,
    spatial_ref,
    bias_ref,
    *rest,
):
    vector_refs, rest = rest[:13], rest[13:]
    layer(
        sizes,
        (stream_ref, vector_refs, spatial_ref, bias_ref),
        (
            first_gate_ref,
            first_up_ref,
            first_down_ref,
            left_ref,
            right_ref,
            mixer_out_ref,
            second_gate_ref,
            second_up_ref,
            second_down_ref,
        ),
        *rest,
    )


def layer(
    sizes,
    inputs,
    weights,
    out_ref,
    tall,
    small,
    vectors_ref,
    w,
    scl,
    scol,
    cols,
    act,
    xn,
    acc,
    hid,
    gated,
    left,
    right,
    pbuf,
    sb,
    pr,
    cb,
    rl,
    rr,
    st,
    st_own,
    in_sem,
    zsend,
    zrecv,
    ssend,
    srecv,
    ysend,
    yrecv,
    psend,
    precv,
    csend,
    crecv,
    lrecv,
    gsend,
    grecv,
    tsend,
    trecv,
):
    nz, ntp, ff, ch, span = sizes
    stream_ref, vector_refs, spatial_ref, bias_ref = inputs
    nx, half = ntp // 2, nz // 2
    hidden_at = vectors_ref.shape[1] - 2 * LANES - (-ff % LANES) - ff
    mixer_at = vectors_ref.shape[1] - 2 * LANES
    scale_at = vectors_ref.shape[1] - LANES
    rows, toks = stream_ref.shape
    g, z, t = lax.axis_index("grp"), lax.axis_index("fs"), lax.axis_index("tp")
    x, c = t // 2, t % 2
    gp = g % 2

    def at_tp(other):
        return (g, z, other)

    partner = (g + 1 - 2 * gp, z, t)
    sibling = at_tp(2 * x + 1 - c)
    xr, xl = (x + 1) % nx, (x + nx - 1) % nx
    right_x, left_x = at_tp(2 * xr + c), at_tp(2 * xl + c)
    around = ((g, (z + 1) % nz, t), (g, (z + nz - 1) % nz, t))

    def copy(src, dst, send, recv, device):
        return pltpu.make_async_remote_copy(
            src_ref=src, dst_ref=dst, send_sem=send, recv_sem=recv, device_id=device, device_id_type=MESH
        )

    third = ff * 15 // 44
    alone = (2 * third, third, ch, 2 * third - 32, third - 48)
    total = (2 * ff, ff, 3 * ch, 2 * ff, ff)
    base, first = [], 0
    for n in total:
        base.append(first)
        first += n

    y_slot = (0, 1, 2, 0, 3)

    def part(p, sub, zs):
        shared = total[p] - 2 * alone[p]
        if sub == 0:
            return w.at[zs, pl.ds(pl.multiple_of(base[p] + gp * (alone[p] + shared), 16), alone[p])]
        return w.at[zs, pl.ds(base[p] + alone[p], shared)]

    def source(d, k):
        return (z + nz - k) % nz if d == 0 else (z + k) % nz

    def last(d, sub):
        return half if d == sub else half - 1

    def hop(p, d, sub, zs, k):
        return copy(part(p, sub, zs), part(p, sub, zs), zsend.at[p], zrecv.at[p % 3, d, sub, k], around[d])

    def scale_hop(d, zs, k):
        return copy(scl.at[zs], scl.at[zs], ssend.at[0], srecv.at[d, k], around[d])

    def across(p, zs, k):
        return copy(part(p, 0, zs), part(p, 0, zs), ysend.at[p], yrecv.at[y_slot[p], k - 1], partner)

    def start_ring(p):
        for sub in (0, 1):
            for d in (0, 1):
                hop(p, d, sub, z, 0).start()

    def tick(p, k):
        for sub in (0, 1):
            for d in (0, 1):
                zs = source(d, k)

                @pl.when(k <= last(d, sub))
                def _():
                    hop(p, d, sub, zs, k - 1).wait_recv()

                @pl.when(k < last(d, sub))
                def _():
                    hop(p, d, sub, zs, k).start()

                if sub == 0:

                    @pl.when(k <= last(d, sub))
                    def _():
                        across(p, zs, k).start()

    def scale_tick(k):
        for d in (0, 1):
            zs = source(d, k)

            @pl.when(k <= last(d, 0))
            def _():
                scale_hop(d, zs, k - 1).wait_recv()

            @pl.when(k < last(d, 0))
            def _():
                scale_hop(d, zs, k).start()

    def pair_of(j):
        return (z + nz - j % half) % nz, (z + j) % nz

    def wait_across(p, j):
        for several in (1, 2):

            @pl.when((j < half) == (several == 2))
            def _():
                pieces = w.at[pl.ds(0, several), pl.ds(base[p], alone[p])]
                copy(pieces, pieces, ysend.at[p], yrecv.at[y_slot[p], j - 1], partner).wait_recv()

    own_rows = pl.ds(pl.multiple_of(t * rows, rows), rows)
    hr = rows // 2

    def chunk(r, tt, h):
        return act.at[r, pl.ds(pl.multiple_of(tt * rows + h * hr, hr), hr)]

    def g_half(r, i, tt, h, device):
        return copy(chunk(r, tt, h), chunk(r, tt, h), gsend.at[r], grecv.at[i if i < 7 else 0], device)

    def g_whole(r):
        return copy(act.at[r, own_rows], act.at[r, own_rows], gsend.at[r], grecv.at[0], sibling)

    far = (x + 2) % nx

    def gather_start(r):
        g_half(r, 1, t, 0, right_x).start()
        g_half(r, 4, t, 1, left_x).start()
        g_half(r, 2, t, 1, right_x).start()
        g_half(r, 3, t, 0, left_x).start()
        g_whole(r).start()

    def gather_middle(r):
        from_left, from_right = 2 * xl + c, 2 * xr + c
        g_half(r, 1, from_left, 0, right_x).wait_recv()
        g_half(r, 5, from_left, 0, right_x).start()
        g_half(r, 7, from_left, 0, sibling).start()
        g_half(r, 4, from_right, 1, left_x).wait_recv()
        g_half(r, 6, from_right, 1, left_x).start()
        g_half(r, 10, from_right, 1, sibling).start()
        g_half(r, 2, from_left, 1, right_x).wait_recv()
        g_half(r, 8, from_left, 1, sibling).start()
        g_half(r, 3, from_right, 0, left_x).wait_recv()
        g_half(r, 9, from_right, 0, sibling).start()

    def gather_end(r):
        g_half(r, 5, 2 * far + c, 0, right_x).wait_recv()
        g_half(r, 11, 2 * far + c, 0, sibling).start()
        g_half(r, 6, 2 * far + c, 1, left_x).wait_recv()
        g_half(r, 12, 2 * far + c, 1, sibling).start()
        arrived = act.at[r, pl.ds(0, 4 * rows)]
        copy(arrived, arrived, gsend.at[r], grecv.at[0], sibling).wait_recv()

    def gather_drain(r):
        sent = act.at[r, pl.ds(0, 7 * rows)]
        copy(sent, sent, gsend.at[r], grecv.at[0], sibling).wait_send()

    def normalise(r):
        def squares(i, s):
            v = act[r, pl.ds(pl.multiple_of(i * LANES, LANES), LANES)].astype(F32)
            return s + jnp.sum(v * v, axis=0, keepdims=True)

        s = lax.fori_loop(0, nz, squares, jnp.zeros((1, toks), F32))
        inverse = lax.rsqrt(s / (rows * ntp) + EPS)

        def apply(i, _):
            at = pl.ds(pl.multiple_of(i * LANES, LANES), LANES)
            v = act[r, at].astype(F32)
            xn[at] = (v * inverse * cols[at, r : r + 1]).astype(BF16)
            return 0

        lax.fori_loop(0, nz, apply, 0)

    def project_pair(at, n, j, piece):
        a, b = pair_of(j)
        rhs = jnp.concatenate(
            [xn[pl.ds(pl.multiple_of(q * LANES, LANES), LANES)] for q in (a, b)], axis=0
        )

        def one(i, _):
            here = pl.ds(pl.multiple_of(at + i * piece, 16), piece)
            lhs = jnp.concatenate([w[a, here], w[b, here]], axis=1)
            got = jnp.dot(lhs, rhs, preferred_element_type=F32)
            there = pl.ds(pl.multiple_of(i * piece, 16), piece)
            acc[there] = acc[there] + got
            return 0

        lax.fori_loop(0, n // piece, one, 0)

    def clear(n):
        def one(i, _):
            acc[pl.ds(pl.multiple_of(i * 64, 64), 64)] = jnp.zeros((64, toks), F32)
            return 0

        lax.fori_loop(0, n // 64, one, 0)

    def hidden(b):
        def one(i, _):
            at = pl.ds(pl.multiple_of(i * 64, 64), 64)
            up_at = pl.ds(pl.multiple_of(ff + i * 64, 64), 64)
            scale = cols[pl.ds(pl.multiple_of(hidden_at + i * 64, 64), 64)]
            gate = acc[at] * scale[:, 2 * b : 2 * b + 1]
            up = acc[up_at] * scale[:, 2 * b + 1 : 2 * b + 2]
            hid[at] = (gate / (1.0 + jnp.exp(-gate)) * up).astype(BF16)
            return 0

        lax.fori_loop(0, ff // 64, one, 0)

    def to_sibling(r, zs):
        return copy(sb.at[r, zs], pr.at[r, zs], psend.at[r], precv.at[zs], sibling)

    def to_owner(r, zs, slot):
        device = (right_x, left_x, at_tp(2 * far + c))[slot - 1]
        return copy(cb.at[r, zs], rr.at[r, slot, zs % 2], csend.at[r], crecv.at[r], device)

    def to_relay(r, zs, side):
        return copy(cb.at[r, zs], rl.at[r, side], csend.at[r], lrecv.at[r, side], (right_x, left_x)[side])

    def produce(r, pieces, lhs, rhs):
        product = contract_rows(lhs, rhs)
        for i, zs in enumerate(pieces):
            col = scol[zs][:, r : r + 1]
            term = product[i * LANES : (i + 1) * LANES] * col
            mine = (zs // 2) % 2 == c

            @pl.when(mine)
            def _():
                pbuf[zs] = term

            @pl.when(jnp.logical_not(mine))
            def _():
                sb[r, zs] = term.astype(BF16)
                to_sibling(r, zs).start()

    def both_cores(r, zs):
        to_sibling(r, zs).wait_recv()
        return pbuf[zs] + pr[r, zs].astype(F32)

    def combine(r, j):
        for zs in pair_of(j):

            @pl.when((zs // 2) % 2 == c)
            def _():
                both = both_cores(r, zs).astype(BF16)

                @pl.when(zs // 4 == x)
                def _():
                    rr[r, 0, zs % 2] = both

                @pl.when(zs // 4 != x)
                def _():
                    cb[r, zs] = both

                for slot, owner in ((1, xr), (2, xl), (3, far)):

                    @pl.when(zs // 4 == owner)
                    def _():
                        to_owner(r, zs, slot).start()

    def turn_of(i):
        away = jnp.where(i < 2, 2, jnp.where(i // 2 == 2, 0, 1 + 2 * (i % 2)))
        return away, (x + away) % nx, jnp.where(i < 6, ((i + 1) // 2) % 2, i % 2)

    def pieces_of(i):
        _, owner, q = turn_of(i)
        return 4 * owner + q, 4 * owner + 2 + q

    def combine_turn(r, i):
        away, owner, q = turn_of(i)
        zs = 4 * owner + 2 * c + q
        both = both_cores(r, zs)

        @pl.when(away == 0)
        def _():
            rr[r, 0, q] = both.astype(BF16)

        for side in (0, 1):

            @pl.when(jnp.logical_and(away == 2, q == side))
            def _():
                cb[r, zs] = both.astype(BF16)
                to_relay(r, zs, side).start()

            @pl.when(jnp.logical_and(away == 1 + 2 * side, q != side))
            def _():
                cb[r, zs] = both.astype(BF16)
                to_owner(r, zs, 1 + side).start()

            @pl.when(jnp.logical_and(away == 1 + 2 * side, q == side))
            def _():
                to_relay(r, zs, side).wait_recv()
                cb[r, zs] = (both + rl[r, side].astype(F32)).astype(BF16)
                to_owner(r, zs, 1 + side).start()

    def finish(r, factor):
        slots = (0, 1, 2, 3) if r == 0 else (0, 1, 2)
        arrived = cb.at[r, pl.ds(0, 2 * len(slots) - 2)]
        copy(arrived, arrived, csend.at[r], crecv.at[r], sibling).wait_recv()
        news = []
        for h in (0, 1):
            summed = rr[r, 0, h].astype(F32)
            for slot in slots[1:]:
                summed = summed + rr[r, slot, h].astype(F32)
            at = pl.ds(pl.multiple_of(t * rows + h * LANES, LANES), LANES)
            news.append((act[r, at].astype(F32) + factor * summed).astype(BF16))
        return news

    def next_stream(r, factor):
        for h, new in enumerate(finish(r, factor)):
            act[r + 1, pl.ds(pl.multiple_of(t * rows + h * LANES, LANES), LANES)] = new

    def reduce_drain(r):
        sent = sb.at[r, pl.ds(0, half)]
        copy(sent, sent, psend.at[r], precv.at[0], sibling).wait_send()
        sent = cb.at[r, pl.ds(0, 2 * (nx - 1))]
        copy(sent, sent, csend.at[r], crecv.at[r], sibling).wait_send()

    def down_piece(p, r, pieces):
        a, b = pieces
        lhs = jnp.concatenate([w[a, pl.ds(base[p], ff)], w[b, pl.ds(base[p], ff)]], axis=1)
        produce(r, pieces, lhs, hid[...])

    fetch_stream = pltpu.make_async_copy(stream_ref, act.at[0, own_rows], in_sem.at[0])
    first_gate, first_up, first_down, left_w, right_w, mixer_out, second_gate, second_up, second_down = weights
    shares = (
        (first_gate, tall.at[0], base[0], False),
        (first_up, tall.at[1], base[0] + ff, False),
        (first_down, tall.at[2], base[1], False),
        (left_w, small.at[0], base[2], True),
        (right_w, small.at[1], base[2] + ch, True),
        (mixer_out, small.at[2], base[2] + 2 * ch, False),
        (second_gate, tall.at[3], base[3], False),
        (second_up, tall.at[4], base[3] + ff, False),
        (second_down, tall.at[5], base[4], False),
    )
    fetches = [
        pltpu.make_async_copy(src, held, in_sem.at[2 + i]) for i, (src, held, _, _) in enumerate(shares)
    ]

    def catch(i):
        fetches[i].wait()
        _, held, at, turned = shares[i]
        if not turned:
            w[z, at : at + held.shape[0]] = held[...].astype(BF16)
            return
        for n in range(0, held.shape[1], LANES):
            wid = min(LANES, held.shape[1] - n)
            w[z, at + n : at + n + wid] = jnp.transpose(held[:, n : n + wid]).astype(BF16)

    fetches[0].start()
    fetches[1].start()
    fetch_stream.start()
    for fetch in fetches[2:]:
        fetch.start()

    barrier = pltpu.get_barrier_semaphore()
    peers = [*around, partner] + [at_tp((t + d) % ntp) for d in range(1, ntp)]
    for device in peers:
        pl.semaphore_signal(barrier, inc=1, device_id=device, device_id_type=MESH)
    vectors_ref[...] = jnp.zeros_like(vectors_ref)
    places = [(i, 0) for i in range(3)] + [(i, hidden_at) for i in range(4)]
    places += [(i, mixer_at) for i in range(3)] + [(i, scale_at) for i in range(3)]
    for ref, (row, at) in zip(vector_refs, places):
        vectors_ref[row : row + 1, at : at + ref.shape[1]] = ref[...]
    scl[z] = vectors_ref[:, scale_at : scale_at + LANES]
    catch(0)
    catch(1)
    pl.semaphore_wait(barrier, len(peers))

    start_ring(0)
    fetch_stream.wait()
    gather_start(0)
    for d in (0, 1):
        scale_hop(d, z, 0).start()
    for i in range(2, 9):
        catch(i)
    clear(2 * ff)

    def turn(i, _):
        at = pl.ds(pl.multiple_of(i * LANES, LANES), LANES)
        cols[at] = jnp.transpose(vectors_ref[:, at])
        return 0

    lax.fori_loop(0, vectors_ref.shape[1] // LANES, turn, 0)
    tick(0, 1)
    gather_middle(0)
    scale_tick(1)
    tick(0, 2)
    gather_end(0)
    normalise(0)

    def first_loop(j, _):
        @pl.when(j + 2 <= half)
        def _():
            tick(0, j + 2)
            scale_tick(j + 1)

        @pl.when(j + 2 == half - 1)
        def _():
            start_ring(1)
            start_ring(2)

        @pl.when(j == half)
        def _():
            tick(1, 1)
            tick(2, 1)

        wait_across(0, j)
        project_pair(base[0], 2 * ff, j, ff // 2)
        return 0

    lax.fori_loop(1, half + 1, first_loop, 0)
    scale_tick(half)
    hidden(0)

    def turn_scale(q, _):
        scol[q] = jnp.transpose(scl[q])
        return 0

    lax.fori_loop(0, nz, turn_scale, 0)

    def inside(j):
        return jnp.logical_and(j >= 1, j <= half)

    def second_loop(j, _):
        @pl.when(j + 1 <= half)
        def _():
            tick(1, j + 1)
            tick(2, j + 1)

        @pl.when(j + 1 == half - 1)
        def _():
            start_ring(3)
            start_ring(4)

        @pl.when(j <= half)
        def _():
            wait_across(1, j)
            down_piece(1, 0, pair_of(j))

        @pl.when(inside(j - 1))
        def _():
            combine(0, j - 1)

        return 0

    lax.fori_loop(1, half + 2, second_loop, 0)
    tick(3, 1)
    next_stream(0, 0.5)
    gather_start(1)
    tick(4, 1)
    tick(3, 2)
    gather_middle(1)
    tick(4, 2)
    gather_end(1)
    normalise(1)
    tick(3, 3)
    clear(2 * ch)

    def mixer_loop(j, _):
        wait_across(2, j)
        project_pair(base[2], 2 * ch, j, 2 * ch)
        return 0

    lax.fori_loop(1, half + 1, mixer_loop, 0)
    mixer_cols = cols[mixer_at : mixer_at + ch]
    left[...] = jax.nn.gelu(acc[0:ch] * mixer_cols[:, 0:1])
    right[...] = jax.nn.gelu(acc[ch : 2 * ch] * mixer_cols[:, 1:2])
    st_own[...] = jnp.zeros_like(st_own)
    st_own[0:1] = jnp.sum(right[...], axis=0, keepdims=True)
    st_own[1:2] = jnp.sum(right[...] * right[...], axis=0, keepdims=True)

    def to_peer(d):
        return copy(st_own, st.at[t], tsend.at[0], trecv.at[0], at_tp((t + d) % ntp))

    for d in range(1, ntp):
        to_peer(d).start()
    tick(4, 3)
    st[t] = st_own[...]
    arrived = st.at[pl.ds(0, ntp - 1)]
    copy(arrived, arrived, tsend.at[0], trecv.at[0], sibling).wait_recv()
    sums = st[0]
    for i in range(1, ntp):
        sums = sums + st[i]
    average = sums[0:1] / (ch * ntp)
    inverse = lax.rsqrt(sums[1:2] / (ch * ntp) - average * average + EPS)
    centred = ((right[...] - average) * inverse * mixer_cols[:, 2:3]).astype(BF16)
    target = lax.broadcasted_iota(jnp.int32, (span, span), 0)
    origin = lax.broadcasted_iota(jnp.int32, (span, span), 1)
    masked = jnp.where(origin <= target, spatial_ref[...].astype(F32), 0.0).astype(BF16)
    for n in range(toks // span):
        at = slice(n * span, (n + 1) * span)
        mixed = lax.dot_general(
            centred[:, at], masked, (((1,), (1,)), ((), ())), preferred_element_type=F32
        )
        gated[:, at] = (left[:, at] * (mixed + bias_ref[...])).astype(BF16)

    def mixer_out_loop(i, _):
        @pl.when(i < half)
        def _():
            a, b = pieces_of(i)
            here = pl.ds(base[2] + 2 * ch, ch)
            produce(1, (a, b), jnp.concatenate([w[a, here], w[b, here]], axis=1), gated[...])

        @pl.when(i >= 3)
        def _():
            combine_turn(1, i - 3)

        @pl.when(i == 3)
        def _():
            tick(3, 4)

        @pl.when(i == half)
        def _():
            tick(4, 4)

        return 0

    lax.fori_loop(0, half + 3, mixer_out_loop, 0)
    tick(3, 5)
    next_stream(1, 1.0)
    gather_start(2)
    tick(4, 5)
    gather_middle(2)
    tick(3, 6)
    gather_end(2)
    normalise(2)
    clear(2 * ff)

    def third_loop(j, _):
        @pl.when(j == 2)
        def _():
            tick(3, half - 1)
            tick(4, half - 2)

        @pl.when(j == half - 3)
        def _():
            tick(3, half)

        @pl.when(j == half - 1)
        def _():
            tick(4, half - 1)

        wait_across(3, j)
        project_pair(base[3], 2 * ff, j, ff // 2)
        return 0

    lax.fori_loop(1, half + 1, third_loop, 0)
    tick(4, half)
    hidden(1)

    for j in range(1, half + 1):
        wait_across(4, j)

    def fourth_loop(i, _):
        @pl.when(i < half)
        def _():
            down_piece(4, 2, pieces_of(i))

        @pl.when(i >= 2)
        def _():
            combine_turn(2, i - 2)

        return 0

    lax.fori_loop(0, half + 2, fourth_loop, 0)
    for h, new in enumerate(finish(2, 0.5)):
        out_ref[h * LANES : (h + 1) * LANES] = new

    for p in range(5):
        sent = w.at[pl.ds(0, nz - 1), pl.ds(base[p], total[p] - alone[p])]
        copy(sent, sent, zsend.at[p], zrecv.at[0, 0, 0, 0], sibling).wait_send()
        sent = w.at[pl.ds(0, nz - 1), pl.ds(base[p], alone[p])]
        copy(sent, sent, ysend.at[p], yrecv.at[0, 0], sibling).wait_send()
    sent = scl.at[pl.ds(0, nz - 1)]
    copy(sent, sent, ssend.at[0], srecv.at[0, 0], sibling).wait_send()
    for r in range(3):
        gather_drain(r)
        reduce_drain(r)
    sent = st.at[pl.ds(0, ntp - 1)]
    copy(sent, sent, tsend.at[0], trecv.at[0], sibling).wait_send()


def solution(mesh):
    nz, ntp = mesh.shape["fs"], mesh.shape["tp"]

    def local(
        stream,
        first_gain,
        first_gate,
        first_gate_scale,
        first_up,
        first_up_scale,
        first_down,
        first_down_scale,
        mixer_gain,
        mixer_left,
        mixer_left_scale,
        mixer_right,
        mixer_right_scale,
        channel_gain,
        spatial,
        spatial_bias,
        mixer_out,
        mixer_out_scale,
        second_gain,
        second_gate,
        second_gate_scale,
        second_up,
        second_up_scale,
        second_down,
        second_down_scale,
    ):
        rows, toks = stream.shape
        width, ff = first_gate.shape
        ch, span = mixer_left.shape[1], spatial.shape[1]
        whole = width * nz
        vectors = [
            v.reshape(1, -1)
            for v in (
                first_gain,
                mixer_gain,
                second_gain,
                first_gate_scale,
                first_up_scale,
                second_gate_scale,
                second_up_scale,
                mixer_left_scale,
                mixer_right_scale,
                channel_gain,
                first_down_scale,
                mixer_out_scale,
                second_down_scale,
            )
        ]
        lanes = whole + ff + -ff % LANES + 2 * LANES
        depth = 6 * ff + 3 * ch
        dma, half = pltpu.SemaphoreType.DMA, nz // 2
        vmem, anywhere = pl.BlockSpec(memory_space=pltpu.VMEM), pl.BlockSpec(memory_space=pl.ANY)
        sizes = (nz, ntp, ff, ch, span)

        def body(*refs):
            kernel(sizes, *refs)

        piece = (nz, LANES, toks)
        return pl.pallas_call(
            body,
            out_shape=jax.ShapeDtypeStruct((rows, toks), BF16),
            in_specs=[anywhere] * 10 + [vmem] * 15,
            out_specs=vmem,
            scratch_shapes=[
                pltpu.VMEM((6, ff, width), F32),
                pltpu.VMEM((3, width, ch), F32),
                pltpu.VMEM((8, lanes), F32),
                pltpu.VMEM((nz, depth, LANES), BF16),
                pltpu.VMEM((nz, 8, LANES), F32),
                pltpu.VMEM((nz, LANES, 8), F32),
                pltpu.VMEM((lanes, 8), F32),
                pltpu.VMEM((3, whole, toks), BF16),
                pltpu.VMEM((whole, toks), BF16),
                pltpu.VMEM((2 * ff, toks), F32),
                pltpu.VMEM((ff, toks), BF16),
                pltpu.VMEM((ch, toks), BF16),
                pltpu.VMEM((ch, toks), F32),
                pltpu.VMEM((ch, toks), F32),
                pltpu.VMEM(piece, F32),
                pltpu.VMEM((3, *piece), BF16),
                pltpu.VMEM((3, *piece), BF16),
                pltpu.VMEM((3, *piece), BF16),
                pltpu.VMEM((3, 2, LANES, toks), BF16),
                pltpu.VMEM((3, 4, 2, LANES, toks), BF16),
                pltpu.VMEM((ntp, 8, toks), F32),
                pltpu.VMEM((8, toks), F32),
                dma((11,)),
                dma((5,)),
                dma((3, 2, 2, half)),
                dma((1,)),
                dma((2, half)),
                dma((5,)),
                dma((4, half)),
                dma((3,)),
                dma((nz,)),
                dma((3,)),
                dma((3,)),
                dma((3, 2)),
                dma((3,)),
                dma((7,)),
                dma((1,)),
                dma((1,)),
            ],
            compiler_params=pltpu.CompilerParams(
                collective_id=0, has_side_effects=True, vmem_limit_bytes=60 * 1024 * 1024
            ),
            name="layer",
        )(
            stream,
            first_gate.T,
            first_up.T,
            first_down,
            mixer_left,
            mixer_right,
            mixer_out,
            second_gate.T,
            second_up.T,
            second_down,
            spatial.reshape(span, span),
            spatial_bias,
            *vectors,
        )

    return jax.shard_map(
        local,
        mesh=mesh,
        in_specs=(
            P("tp", ("grp", "fs")),
            P(),
            P("fs", "tp"),
            P("tp"),
            P("fs", "tp"),
            P("tp"),
            P("tp", "fs"),
            P("fs"),
            P(),
            P("fs", "tp"),
            P("tp"),
            P("fs", "tp"),
            P("tp"),
            P("tp"),
            P("tp", None, None),
            P("tp", None),
            P("tp", "fs"),
            P("fs"),
            P(),
            P("fs", "tp"),
            P("tp"),
            P("fs", "tp"),
            P("tp"),
            P("tp", "fs"),
            P("fs"),
        ),
        out_specs=P("tp", ("grp", "fs")),
        check_vma=False,
    )
```

```python
import jax
import jax.numpy as jnp
from jax import lax
from jax.experimental import pallas as pl
from jax.experimental.pallas import tpu as pltpu
from jax.sharding import PartitionSpec as P

MESH = pl.DeviceIdType.MESH
EPS = 1e-06
F32, BF16 = jnp.float32, jnp.bfloat16
LANES = 128


def contract_rows(a, b):
    return lax.dot_general(a, b, (((0,), (0,)), ((), ())), preferred_element_type=F32)


def kernel(
    sizes,
    stream_ref,
    first_gate_ref,
    first_up_ref,
    first_down_ref,
    left_ref,
    right_ref,
    mixer_out_ref,
    second_gate_ref,
    second_up_ref,
    second_down_ref,
    spatial_ref,
    bias_ref,
    *rest,
):
    vector_refs, rest = rest[:13], rest[13:]
    layer(
        sizes,
        (stream_ref, vector_refs, spatial_ref, bias_ref),
        (
            first_gate_ref,
            first_up_ref,
            first_down_ref,
            left_ref,
            right_ref,
            mixer_out_ref,
            second_gate_ref,
            second_up_ref,
            second_down_ref,
        ),
        *rest,
    )


def layer(
    sizes,
    inputs,
    weights,
    out_ref,
    tall,
    small,
    vectors_ref,
    w,
    scl,
    scol,
    cols,
    act,
    xn,
    acc,
    hid,
    gated,
    left,
    right,
    pbuf,
    sb,
    pr,
    cb,
    rl,
    rr,
    st,
    st_own,
    in_sem,
    zsend,
    zrecv,
    ssend,
    srecv,
    ysend,
    yrecv,
    psend,
    precv,
    csend,
    crecv,
    lrecv,
    gsend,
    grecv,
    tsend,
    trecv,
):
    nz, ntp, ff, ch, span = sizes
    stream_ref, vector_refs, spatial_ref, bias_ref = inputs
    nx, half = ntp // 2, nz // 2
    hidden_at = vectors_ref.shape[1] - 2 * LANES - (-ff % LANES) - ff
    mixer_at = vectors_ref.shape[1] - 2 * LANES
    scale_at = vectors_ref.shape[1] - LANES
    rows, toks = stream_ref.shape
    g, z, t = lax.axis_index("grp"), lax.axis_index("fs"), lax.axis_index("tp")
    x, c = t // 2, t % 2
    gp = g % 2

    def at_tp(other):
        return (g, z, other)

    partner = (g + 1 - 2 * gp, z, t)
    sibling = at_tp(2 * x + 1 - c)
    xr, xl = (x + 1) % nx, (x + nx - 1) % nx
    right_x, left_x = at_tp(2 * xr + c), at_tp(2 * xl + c)
    around = ((g, (z + 1) % nz, t), (g, (z + nz - 1) % nz, t))

    def copy(src, dst, send, recv, device):
        return pltpu.make_async_remote_copy(
            src_ref=src, dst_ref=dst, send_sem=send, recv_sem=recv, device_id=device, device_id_type=MESH
        )

    third = ff * 15 // 44
    alone = (2 * third, third, ch, 2 * third - 32, third - 48)
    total = (2 * ff, ff, 3 * ch, 2 * ff, ff)
    base, first = [], 0
    for n in total:
        base.append(first)
        first += n

    y_slot = (0, 1, 2, 0, 3)

    def part(p, sub, zs):
        shared = total[p] - 2 * alone[p]
        if sub == 0:
            return w.at[zs, pl.ds(pl.multiple_of(base[p] + gp * (alone[p] + shared), 16), alone[p])]
        return w.at[zs, pl.ds(base[p] + alone[p], shared)]

    def source(d, k):
        return (z + nz - k) % nz if d == 0 else (z + k) % nz

    def last(d, sub):
        return half if d == sub else half - 1

    def hop(p, d, sub, zs, k):
        return copy(part(p, sub, zs), part(p, sub, zs), zsend.at[p], zrecv.at[p % 3, d, sub, k], around[d])

    def scale_hop(d, zs, k):
        return copy(scl.at[zs], scl.at[zs], ssend.at[0], srecv.at[d, k], around[d])

    def across(p, zs, k):
        return copy(part(p, 0, zs), part(p, 0, zs), ysend.at[p], yrecv.at[y_slot[p], k - 1], partner)

    def start_ring(p):
        for sub in (0, 1):
            for d in (0, 1):
                hop(p, d, sub, z, 0).start()

    def tick(p, k):
        for sub in (0, 1):
            for d in (0, 1):
                zs = source(d, k)

                @pl.when(k <= last(d, sub))
                def _():
                    hop(p, d, sub, zs, k - 1).wait_recv()

                @pl.when(k < last(d, sub))
                def _():
                    hop(p, d, sub, zs, k).start()

                if sub == 0:

                    @pl.when(k <= last(d, sub))
                    def _():
                        across(p, zs, k).start()

    def scale_tick(k):
        for d in (0, 1):
            zs = source(d, k)

            @pl.when(k <= last(d, 0))
            def _():
                scale_hop(d, zs, k - 1).wait_recv()

            @pl.when(k < last(d, 0))
            def _():
                scale_hop(d, zs, k).start()

    def pair_of(j):
        return (z + nz - j % half) % nz, (z + j) % nz

    def wait_across(p, j):
        for several in (1, 2):

            @pl.when((j < half) == (several == 2))
            def _():
                pieces = w.at[pl.ds(0, several), pl.ds(base[p], alone[p])]
                copy(pieces, pieces, ysend.at[p], yrecv.at[y_slot[p], j - 1], partner).wait_recv()

    own_rows = pl.ds(pl.multiple_of(t * rows, rows), rows)
    hr = rows // 2

    def chunk(r, tt, h):
        return act.at[r, pl.ds(pl.multiple_of(tt * rows + h * hr, hr), hr)]

    def g_half(r, i, tt, h, device):
        return copy(chunk(r, tt, h), chunk(r, tt, h), gsend.at[r], grecv.at[i if i < 7 else 0], device)

    def g_whole(r):
        return copy(act.at[r, own_rows], act.at[r, own_rows], gsend.at[r], grecv.at[0], sibling)

    far = (x + 2) % nx

    def gather_start(r):
        g_half(r, 1, t, 0, right_x).start()
        g_half(r, 4, t, 1, left_x).start()
        g_half(r, 2, t, 1, right_x).start()
        g_half(r, 3, t, 0, left_x).start()
        g_whole(r).start()

    def gather_middle(r):
        from_left, from_right = 2 * xl + c, 2 * xr + c
        g_half(r, 1, from_left, 0, right_x).wait_recv()
        g_half(r, 5, from_left, 0, right_x).start()
        g_half(r, 7, from_left, 0, sibling).start()
        g_half(r, 4, from_right, 1, left_x).wait_recv()
        g_half(r, 6, from_right, 1, left_x).start()
        g_half(r, 10, from_right, 1, sibling).start()
        g_half(r, 2, from_left, 1, right_x).wait_recv()
        g_half(r, 8, from_left, 1, sibling).start()
        g_half(r, 3, from_right, 0, left_x).wait_recv()
        g_half(r, 9, from_right, 0, sibling).start()

    def gather_end(r):
        g_half(r, 5, 2 * far + c, 0, right_x).wait_recv()
        g_half(r, 11, 2 * far + c, 0, sibling).start()
        g_half(r, 6, 2 * far + c, 1, left_x).wait_recv()
        g_half(r, 12, 2 * far + c, 1, sibling).start()
        arrived = act.at[r, pl.ds(0, 4 * rows)]
        copy(arrived, arrived, gsend.at[r], grecv.at[0], sibling).wait_recv()

    def gather_drain(r):
        sent = act.at[r, pl.ds(0, 7 * rows)]
        copy(sent, sent, gsend.at[r], grecv.at[0], sibling).wait_send()

    def normalise(r):
        def squares(i, s):
            v = act[r, pl.ds(pl.multiple_of(i * LANES, LANES), LANES)].astype(F32)
            return s + jnp.sum(v * v, axis=0, keepdims=True)

        s = lax.fori_loop(0, nz, squares, jnp.zeros((1, toks), F32))
        inverse = lax.rsqrt(s / (rows * ntp) + EPS)

        def apply(i, _):
            at = pl.ds(pl.multiple_of(i * LANES, LANES), LANES)
            v = act[r, at].astype(F32)
            xn[at] = (v * inverse * cols[at, r : r + 1]).astype(BF16)
            return 0

        lax.fori_loop(0, nz, apply, 0)

    def project_pair(at, n, j, piece):
        a, b = pair_of(j)
        rhs = jnp.concatenate(
            [xn[pl.ds(pl.multiple_of(q * LANES, LANES), LANES)] for q in (a, b)], axis=0
        )

        def one(i, _):
            here = pl.ds(pl.multiple_of(at + i * piece, 16), piece)
            lhs = jnp.concatenate([w[a, here], w[b, here]], axis=1)
            got = jnp.dot(lhs, rhs, preferred_element_type=F32)
            there = pl.ds(pl.multiple_of(i * piece, 16), piece)
            acc[there] = acc[there] + got
            return 0

        lax.fori_loop(0, n // piece, one, 0)

    def clear(n):
        def one(i, _):
            acc[pl.ds(pl.multiple_of(i * 64, 64), 64)] = jnp.zeros((64, toks), F32)
            return 0

        lax.fori_loop(0, n // 64, one, 0)

    def hidden(b):
        def one(i, _):
            at = pl.ds(pl.multiple_of(i * 64, 64), 64)
            up_at = pl.ds(pl.multiple_of(ff + i * 64, 64), 64)
            scale = cols[pl.ds(pl.multiple_of(hidden_at + i * 64, 64), 64)]
            gate = acc[at] * scale[:, 2 * b : 2 * b + 1]
            up = acc[up_at] * scale[:, 2 * b + 1 : 2 * b + 2]
            hid[at] = (gate / (1.0 + jnp.exp(-gate)) * up).astype(BF16)
            return 0

        lax.fori_loop(0, ff // 64, one, 0)

    def to_sibling(r, zs):
        return copy(sb.at[r, zs], pr.at[r, zs], psend.at[r], precv.at[zs], sibling)

    def to_owner(r, zs, slot):
        device = (right_x, left_x, at_tp(2 * far + c))[slot - 1]
        return copy(cb.at[r, zs], rr.at[r, slot, zs % 2], csend.at[r], crecv.at[r], device)

    def to_relay(r, zs, side):
        return copy(cb.at[r, zs], rl.at[r, side], csend.at[r], lrecv.at[r, side], (right_x, left_x)[side])

    def produce(r, pieces, lhs, rhs):
        product = contract_rows(lhs, rhs)
        for i, zs in enumerate(pieces):
            col = scol[zs][:, r : r + 1]
            term = product[i * LANES : (i + 1) * LANES] * col
            mine = (zs // 2) % 2 == c

            @pl.when(mine)
            def _():
                pbuf[zs] = term

            @pl.when(jnp.logical_not(mine))
            def _():
                sb[r, zs] = term.astype(BF16)
                to_sibling(r, zs).start()

    def both_cores(r, zs):
        to_sibling(r, zs).wait_recv()
        return pbuf[zs] + pr[r, zs].astype(F32)

    def combine(r, j):
        for zs in pair_of(j):

            @pl.when((zs // 2) % 2 == c)
            def _():
                both = both_cores(r, zs).astype(BF16)

                @pl.when(zs // 4 == x)
                def _():
                    rr[r, 0, zs % 2] = both

                @pl.when(zs // 4 != x)
                def _():
                    cb[r, zs] = both

                for slot, owner in ((1, xr), (2, xl), (3, far)):

                    @pl.when(zs // 4 == owner)
                    def _():
                        to_owner(r, zs, slot).start()

    def turn_of(i):
        away = jnp.where(i < 2, 2, jnp.where(i // 2 == 2, 0, 1 + 2 * (i % 2)))
        return away, (x + away) % nx, jnp.where(i < 6, ((i + 1) // 2) % 2, i % 2)

    def pieces_of(i):
        _, owner, q = turn_of(i)
        return 4 * owner + q, 4 * owner + 2 + q

    def combine_turn(r, i):
        away, owner, q = turn_of(i)
        zs = 4 * owner + 2 * c + q
        both = both_cores(r, zs)

        @pl.when(away == 0)
        def _():
            rr[r, 0, q] = both.astype(BF16)

        for side in (0, 1):

            @pl.when(jnp.logical_and(away == 2, q == side))
            def _():
                cb[r, zs] = both.astype(BF16)
                to_relay(r, zs, side).start()

            @pl.when(jnp.logical_and(away == 1 + 2 * side, q != side))
            def _():
                cb[r, zs] = both.astype(BF16)
                to_owner(r, zs, 1 + side).start()

            @pl.when(jnp.logical_and(away == 1 + 2 * side, q == side))
            def _():
                to_relay(r, zs, side).wait_recv()
                cb[r, zs] = (both + rl[r, side].astype(F32)).astype(BF16)
                to_owner(r, zs, 1 + side).start()

    def finish(r, factor):
        slots = (0, 1, 2, 3) if r == 0 else (0, 1, 2)
        arrived = cb.at[r, pl.ds(0, 2 * len(slots) - 2)]
        copy(arrived, arrived, csend.at[r], crecv.at[r], sibling).wait_recv()
        news = []
        for h in (0, 1):
            summed = rr[r, 0, h].astype(F32)
            for slot in slots[1:]:
                summed = summed + rr[r, slot, h].astype(F32)
            at = pl.ds(pl.multiple_of(t * rows + h * LANES, LANES), LANES)
            news.append((act[r, at].astype(F32) + factor * summed).astype(BF16))
        return news

    def next_stream(r, factor):
        for h, new in enumerate(finish(r, factor)):
            act[r + 1, pl.ds(pl.multiple_of(t * rows + h * LANES, LANES), LANES)] = new

    def reduce_drain(r):
        sent = sb.at[r, pl.ds(0, half)]
        copy(sent, sent, psend.at[r], precv.at[0], sibling).wait_send()
        sent = cb.at[r, pl.ds(0, 2 * (nx - 1))]
        copy(sent, sent, csend.at[r], crecv.at[r], sibling).wait_send()

    def down_piece(p, r, pieces):
        a, b = pieces
        lhs = jnp.concatenate([w[a, pl.ds(base[p], ff)], w[b, pl.ds(base[p], ff)]], axis=1)
        produce(r, pieces, lhs, hid[...])

    fetch_stream = pltpu.make_async_copy(stream_ref, act.at[0, own_rows], in_sem.at[0])
    first_gate, first_up, first_down, left_w, right_w, mixer_out, second_gate, second_up, second_down = weights
    shares = (
        (first_gate, tall.at[0], base[0], False),
        (first_up, tall.at[1], base[0] + ff, False),
        (first_down, tall.at[2], base[1], False),
        (left_w, small.at[0], base[2], True),
        (right_w, small.at[1], base[2] + ch, True),
        (mixer_out, small.at[2], base[2] + 2 * ch, False),
        (second_gate, tall.at[3], base[3], False),
        (second_up, tall.at[4], base[3] + ff, False),
        (second_down, tall.at[5], base[4], False),
    )
    fetches = [
        pltpu.make_async_copy(src, held, in_sem.at[2 + i]) for i, (src, held, _, _) in enumerate(shares)
    ]

    def catch(i):
        fetches[i].wait()
        _, held, at, turned = shares[i]
        if not turned:
            w[z, at : at + held.shape[0]] = held[...].astype(BF16)
            return
        for n in range(0, held.shape[1], LANES):
            wid = min(LANES, held.shape[1] - n)
            w[z, at + n : at + n + wid] = jnp.transpose(held[:, n : n + wid]).astype(BF16)

    fetches[0].start()
    fetches[1].start()
    fetch_stream.start()
    for fetch in fetches[2:]:
        fetch.start()

    barrier = pltpu.get_barrier_semaphore()
    peers = [*around, partner] + [at_tp((t + d) % ntp) for d in range(1, ntp)]
    for device in peers:
        pl.semaphore_signal(barrier, inc=1, device_id=device, device_id_type=MESH)
    vectors_ref[...] = jnp.zeros_like(vectors_ref)
    places = [(i, 0) for i in range(3)] + [(i, hidden_at) for i in range(4)]
    places += [(i, mixer_at) for i in range(3)] + [(i, scale_at) for i in range(3)]
    for ref, (row, at) in zip(vector_refs, places):
        vectors_ref[row, at : at + ref.shape[0]] = ref[...]
    scl[z] = vectors_ref[:, scale_at : scale_at + LANES]
    catch(0)
    catch(1)
    pl.semaphore_wait(barrier, len(peers))

    start_ring(0)
    fetch_stream.wait()
    gather_start(0)
    for d in (0, 1):
        scale_hop(d, z, 0).start()
    for i in range(2, 9):
        catch(i)
    clear(2 * ff)

    def turn(i, _):
        at = pl.ds(pl.multiple_of(i * LANES, LANES), LANES)
        cols[at] = jnp.transpose(vectors_ref[:, at])
        return 0

    lax.fori_loop(0, vectors_ref.shape[1] // LANES, turn, 0)
    tick(0, 1)
    gather_middle(0)
    scale_tick(1)
    tick(0, 2)
    gather_end(0)
    normalise(0)

    def first_loop(j, _):
        @pl.when(j + 2 <= half)
        def _():
            tick(0, j + 2)
            scale_tick(j + 1)

        @pl.when(j + 2 == half - 1)
        def _():
            start_ring(1)
            start_ring(2)

        @pl.when(j == half)
        def _():
            tick(1, 1)
            tick(2, 1)

        wait_across(0, j)
        project_pair(base[0], 2 * ff, j, ff // 2)
        return 0

    lax.fori_loop(1, half + 1, first_loop, 0)
    scale_tick(half)
    hidden(0)

    def turn_scale(q, _):
        scol[q] = jnp.transpose(scl[q])
        return 0

    lax.fori_loop(0, nz, turn_scale, 0)

    def inside(j):
        return jnp.logical_and(j >= 1, j <= half)

    def second_loop(j, _):
        @pl.when(j + 1 <= half)
        def _():
            tick(1, j + 1)
            tick(2, j + 1)

        @pl.when(j + 1 == half - 1)
        def _():
            start_ring(3)
            start_ring(4)

        @pl.when(j <= half)
        def _():
            wait_across(1, j)
            down_piece(1, 0, pair_of(j))

        @pl.when(inside(j - 1))
        def _():
            combine(0, j - 1)

        return 0

    lax.fori_loop(1, half + 2, second_loop, 0)
    tick(3, 1)
    next_stream(0, 0.5)
    gather_start(1)
    tick(4, 1)
    tick(3, 2)
    gather_middle(1)
    tick(4, 2)
    gather_end(1)
    normalise(1)
    tick(3, 3)
    clear(2 * ch)

    def mixer_loop(j, _):
        wait_across(2, j)
        project_pair(base[2], 2 * ch, j, 2 * ch)
        return 0

    lax.fori_loop(1, half + 1, mixer_loop, 0)
    mixer_cols = cols[mixer_at : mixer_at + ch]
    left[...] = jax.nn.gelu(acc[0:ch] * mixer_cols[:, 0:1])
    right[...] = jax.nn.gelu(acc[ch : 2 * ch] * mixer_cols[:, 1:2])
    st_own[...] = jnp.zeros_like(st_own)
    st_own[0:1] = jnp.sum(right[...], axis=0, keepdims=True)
    st_own[1:2] = jnp.sum(right[...] * right[...], axis=0, keepdims=True)

    def to_peer(d):
        return copy(st_own, st.at[t], tsend.at[0], trecv.at[0], at_tp((t + d) % ntp))

    for d in range(1, ntp):
        to_peer(d).start()
    tick(4, 3)
    st[t] = st_own[...]
    arrived = st.at[pl.ds(0, ntp - 1)]
    copy(arrived, arrived, tsend.at[0], trecv.at[0], sibling).wait_recv()
    sums = st[0]
    for i in range(1, ntp):
        sums = sums + st[i]
    average = sums[0:1] / (ch * ntp)
    inverse = lax.rsqrt(sums[1:2] / (ch * ntp) - average * average + EPS)
    centred = ((right[...] - average) * inverse * mixer_cols[:, 2:3]).astype(BF16)
    target = lax.broadcasted_iota(jnp.int32, (span, span), 0)
    origin = lax.broadcasted_iota(jnp.int32, (span, span), 1)
    masked = jnp.where(origin <= target, spatial_ref[...].astype(F32), 0.0).astype(BF16)
    for n in range(toks // span):
        at = slice(n * span, (n + 1) * span)
        mixed = lax.dot_general(
            centred[:, at], masked, (((1,), (1,)), ((), ())), preferred_element_type=F32
        )
        gated[:, at] = (left[:, at] * (mixed + bias_ref[...])).astype(BF16)

    def mixer_out_loop(i, _):
        @pl.when(i < half)
        def _():
            a, b = pieces_of(i)
            here = pl.ds(base[2] + 2 * ch, ch)
            produce(1, (a, b), jnp.concatenate([w[a, here], w[b, here]], axis=1), gated[...])

        @pl.when(i >= 3)
        def _():
            combine_turn(1, i - 3)

        @pl.when(i == 3)
        def _():
            tick(3, 4)

        @pl.when(i == half)
        def _():
            tick(4, 4)

        return 0

    lax.fori_loop(0, half + 3, mixer_out_loop, 0)
    tick(3, 5)
    next_stream(1, 1.0)
    gather_start(2)
    tick(4, 5)
    gather_middle(2)
    tick(3, 6)
    gather_end(2)
    normalise(2)
    clear(2 * ff)

    def third_loop(j, _):
        @pl.when(j == 2)
        def _():
            tick(3, half - 1)
            tick(4, half - 2)

        @pl.when(j == half - 3)
        def _():
            tick(3, half)

        @pl.when(j == half - 1)
        def _():
            tick(4, half - 1)

        wait_across(3, j)
        project_pair(base[3], 2 * ff, j, ff // 2)
        return 0

    lax.fori_loop(1, half + 1, third_loop, 0)
    tick(4, half)
    hidden(1)

    for j in range(1, half + 1):
        wait_across(4, j)

    def fourth_loop(i, _):
        @pl.when(i < half)
        def _():
            down_piece(4, 2, pieces_of(i))

        @pl.when(i >= 2)
        def _():
            combine_turn(2, i - 2)

        return 0

    lax.fori_loop(0, half + 2, fourth_loop, 0)
    for h, new in enumerate(finish(2, 0.5)):
        out_ref[h * LANES : (h + 1) * LANES] = new

    for p in range(5):
        sent = w.at[pl.ds(0, nz - 1), pl.ds(base[p], total[p] - alone[p])]
        copy(sent, sent, zsend.at[p], zrecv.at[0, 0, 0, 0], sibling).wait_send()
        sent = w.at[pl.ds(0, nz - 1), pl.ds(base[p], alone[p])]
        copy(sent, sent, ysend.at[p], yrecv.at[0, 0], sibling).wait_send()
    sent = scl.at[pl.ds(0, nz - 1)]
    copy(sent, sent, ssend.at[0], srecv.at[0, 0], sibling).wait_send()
    for r in range(3):
        gather_drain(r)
        reduce_drain(r)
    sent = st.at[pl.ds(0, ntp - 1)]
    copy(sent, sent, tsend.at[0], trecv.at[0], sibling).wait_send()


def solution(mesh):
    nz, ntp = mesh.shape["fs"], mesh.shape["tp"]

    def local(
        stream,
        first_gain,
        first_gate,
        first_gate_scale,
        first_up,
        first_up_scale,
        first_down,
        first_down_scale,
        mixer_gain,
        mixer_left,
        mixer_left_scale,
        mixer_right,
        mixer_right_scale,
        channel_gain,
        spatial,
        spatial_bias,
        mixer_out,
        mixer_out_scale,
        second_gain,
        second_gate,
        second_gate_scale,
        second_up,
        second_up_scale,
        second_down,
        second_down_scale,
    ):
        rows, toks = stream.shape
        width, ff = first_gate.shape
        ch, span = mixer_left.shape[1], spatial.shape[1]
        whole = width * nz
        vectors = [
            v
            for v in (
                first_gain,
                mixer_gain,
                second_gain,
                first_gate_scale,
                first_up_scale,
                second_gate_scale,
                second_up_scale,
                mixer_left_scale,
                mixer_right_scale,
                channel_gain,
                first_down_scale,
                mixer_out_scale,
                second_down_scale,
            )
        ]
        lanes = whole + ff + -ff % LANES + 2 * LANES
        depth = 6 * ff + 3 * ch
        dma, half = pltpu.SemaphoreType.DMA, nz // 2
        vmem, anywhere = pl.BlockSpec(memory_space=pltpu.VMEM), pl.BlockSpec(memory_space=pl.ANY)
        sizes = (nz, ntp, ff, ch, span)

        def body(*refs):
            kernel(sizes, *refs)

        piece = (nz, LANES, toks)
        return pl.pallas_call(
            body,
            out_shape=jax.ShapeDtypeStruct((rows, toks), BF16),
            in_specs=[anywhere] * 10 + [vmem] * 15,
            out_specs=vmem,
            scratch_shapes=[
                pltpu.VMEM((6, ff, width), F32),
                pltpu.VMEM((3, width, ch), F32),
                pltpu.VMEM((8, lanes), F32),
                pltpu.VMEM((nz, depth, LANES), BF16),
                pltpu.VMEM((nz, 8, LANES), F32),
                pltpu.VMEM((nz, LANES, 8), F32),
                pltpu.VMEM((lanes, 8), F32),
                pltpu.VMEM((3, whole, toks), BF16),
                pltpu.VMEM((whole, toks), BF16),
                pltpu.VMEM((2 * ff, toks), F32),
                pltpu.VMEM((ff, toks), BF16),
                pltpu.VMEM((ch, toks), BF16),
                pltpu.VMEM((ch, toks), F32),
                pltpu.VMEM((ch, toks), F32),
                pltpu.VMEM(piece, F32),
                pltpu.VMEM((3, *piece), BF16),
                pltpu.VMEM((3, *piece), BF16),
                pltpu.VMEM((3, *piece), BF16),
                pltpu.VMEM((3, 2, LANES, toks), BF16),
                pltpu.VMEM((3, 4, 2, LANES, toks), BF16),
                pltpu.VMEM((ntp, 8, toks), F32),
                pltpu.VMEM((8, toks), F32),
                dma((11,)),
                dma((5,)),
                dma((3, 2, 2, half)),
                dma((1,)),
                dma((2, half)),
                dma((5,)),
                dma((4, half)),
                dma((3,)),
                dma((nz,)),
                dma((3,)),
                dma((3,)),
                dma((3, 2)),
                dma((3,)),
                dma((7,)),
                dma((1,)),
                dma((1,)),
            ],
            compiler_params=pltpu.CompilerParams(
                collective_id=0, has_side_effects=True, vmem_limit_bytes=60 * 1024 * 1024
            ),
            name="layer",
        )(
            stream,
            first_gate.T,
            first_up.T,
            first_down,
            mixer_left,
            mixer_right,
            mixer_out,
            second_gate.T,
            second_up.T,
            second_down,
            spatial.reshape(span, span),
            spatial_bias,
            *vectors,
        )

    return jax.shard_map(
        local,
        mesh=mesh,
        in_specs=(
            P("tp", ("grp", "fs")),
            P(),
            P("fs", "tp"),
            P("tp"),
            P("fs", "tp"),
            P("tp"),
            P("tp", "fs"),
            P("fs"),
            P(),
            P("fs", "tp"),
            P("tp"),
            P("fs", "tp"),
            P("tp"),
            P("tp"),
            P("tp", None, None),
            P("tp", None),
            P("tp", "fs"),
            P("fs"),
            P(),
            P("fs", "tp"),
            P("tp"),
            P("fs", "tp"),
            P("tp"),
            P("tp", "fs"),
            P("fs"),
        ),
        out_specs=P("tp", ("grp", "fs")),
        check_vma=False,
    )
```
